256 devices in a mesh: ep: 64 (over z, x, core), tp: 4 (over y).
Axes of the slice: x: 4, y: 4, z: 8, core: 2. Of those that a mesh axis runs over, the one named last changes fastest.
Arguments:
- tokens: bfloat16 [16384, 2048], P('ep'), may hold values from -6 to 6
- routes: int32 [16384, 4], P('ep'), may hold values from 0 to 63, all different within a row; in each aligned block of 256 rows (0 to 255, 256 to 511, ...) at most 20 rows name the same one
- gate_weights: float32 [16384, 4], P('ep'), may hold values from 0.05 to 1
- out_grad: bfloat16 [16384, 2048], P('ep'), may hold values from -0.59765625 to 0.59765625
- w_gate: bfloat16 [64, 2048, 1024], P('ep', None, 'tp'), may hold values from -0.1875 to 0.1875
- w_up: bfloat16 [64, 2048, 1024], P('ep', None, 'tp'), may hold values from -0.1875 to 0.1875
- w_down: bfloat16 [64, 1024, 2048], P('ep', 'tp'), may hold values from -0.1875 to 0.1875
Outputs:
- token_grad: bfloat16 [16384, 2048], P('ep', 'tp')
- gate_grad: float32 [16384, 4], P('ep')
- gate_weight_grad: float32 [64, 2048, 1024], P('ep', None, 'tp')
- up_weight_grad: float32 [64, 2048, 1024], P('ep', None, 'tp')
- down_weight_grad: float32 [64, 1024, 2048], P('ep', 'tp')
The draws below stay inside these ranges and needn't reach their ends.
Inputs may be any that keep to these rules, and one draw needn't show every extreme that they name: `routes`: each row names 4 different experts. In each aligned block of 256 rows (the rows of one device) no expert is named by more than 20 rows, and in some block an expert is named by exactly 20 rows.
All inputs are finite; a program needn't handle non-finite values.
Results may differ from the reference program's by a relative error of at most 0.012.
Values may be sent and summed in bfloat16 or wider, within the bound.
A program may use at most 128 MiB of HBM per device.

```python
import math
import jax
import jax.numpy as jnp
import numpy as np
from jax import lax

D = 2048
FF = 1024
TOPK = 4
TOK_DEV = 256
EXPERTS = 64
TOKENS = 16384
CAP = 20
N_EP = 64
N_TP = 4


def steps_of(rng, extent, split, smallest, high):
    def one(axis_at, parts):
        heights = jax.random.uniform(jax.random.fold_in(jax.random.fold_in(rng, 6), axis_at), (parts,), jnp.float32, smallest / len(split), high / len(split))
        return jnp.repeat(jnp.exp(heights), extent[axis_at] // parts).reshape((-1,) + (1,) * (len(extent) - axis_at - 1))

    gain = one(*split[0])
    for cut in split[1:]:
        gain = gain * one(*cut)
    return gain


def assign_block(key, own, number, rows, amount, top, reach, lean):
    ranking = jax.random.permutation(key, amount)
    crowded, usual = portions_of(amount, rows * top, reach, lean, True), portions_of(amount, rows * top, reach, lean, False)
    places = jnp.arange(amount)

    def named(sizes, rotation):
        used = int((sizes > 0).sum())
        fixed = max(1, used // 4)
        moved = fixed + (places - fixed + rotation * (used - fixed)) % max(1, amount - fixed)
        return jnp.zeros((amount,), jnp.int32).at[ranking[jnp.where(places < fixed, places, moved)]].set(jnp.asarray(sizes, jnp.int32))

    sizes = jnp.where(number % 4 == 0, named(crowded, number // 4), named(usual, number - number // 4 - 1))
    mixed = jax.random.permutation(jax.random.fold_in(own, 3), amount)
    source_of, receiver = mixed[0:amount // 2 * 2:2], mixed[1:amount // 2 * 2:2]
    margin = jnp.minimum(sizes[source_of] - 1, reach - sizes[receiver]) // 2
    margin = jnp.where((source_of == ranking[0]) | (receiver == ranking[0]) | (sizes[receiver] == 0), 0, jnp.maximum(margin, 0))
    moved = jax.random.randint(jax.random.fold_in(own, 4), (amount // 2,), 0, 1 << 20) % (margin + 1)
    sizes = sizes.at[source_of].add(-moved).at[receiver].add(moved)
    labels = jnp.searchsorted(jnp.cumsum(sizes), jnp.arange(rows * top), side="right").astype(jnp.int32)
    grid = labels.reshape(top, rows).T
    grid = grid[jax.random.permutation(jax.random.fold_in(own, 1), rows)]
    rotation = jax.random.randint(jax.random.fold_in(own, 2), (rows, 1), 0, top)
    return jnp.take_along_axis(grid, (jnp.arange(top)[None, :] + rotation) % top, axis=1)


def portions_of(count, total, reach, lean, full):
    weights = [(1 << 20) // math.isqrt(rank ** lean) + 1 for rank in range(1, count + 1)]
    largest = reach if full else min(reach, max(-(-total // count), total * weights[0] // sum(weights)))
    least = 1 if total - largest >= count - 1 else 0
    given, surplus = [largest] + [least] * (count - 1), total - largest - least * (count - 1)
    while surplus > 0:
        movable = [i for i in range(1, count) if given[i] < largest] or [i for i in range(1, count) if given[i] < reach]
        mass, remaining = sum([weights[i] for i in movable]), surplus
        for i in movable:
            more = min(reach - given[i], max(1, remaining * weights[i] // mass), surplus)
            given[i] = given[i] + more
            surplus = surplus - more
    return np.array(given)


def bell_draw(key, extent, scale, bound, shards=(), kind=jnp.bfloat16):
    values = jax.random.normal(key, extent, jnp.float32) * scale
    if len(shards) > 0:
        values = steps_of(key, extent, shards, -0.22, 0.18) * values
    return jnp.clip(values, min=-bound, max=bound).astype(kind)


def setup_inputs(seed: int = 0) -> dict:
    key_of = jax.random.split(jax.random.key(seed), 8)
    tokens = bell_draw(key_of[0], (TOKENS, D), 1.0, 6.0, ((0, 64),))
    routes_keys = jax.random.split(jax.random.fold_in(key_of[1], 1), TOKENS // TOK_DEV)
    routes_turns = jax.random.permutation(jax.random.fold_in(key_of[1], 3), TOKENS // TOK_DEV)
    routes = jax.vmap(lambda own, number: assign_block(jax.random.fold_in(key_of[1], 2), own, number, TOK_DEV, EXPERTS, TOPK, CAP, 1))(routes_keys, routes_turns).reshape((TOKENS, TOPK))
    gate_weights = jnp.clip(jnp.exp(math.log(1.0) - 2.9957323 * jax.random.uniform(key_of[2], (TOKENS, TOPK), jnp.float32) ** steps_of(key_of[2], (TOKENS, TOPK), ((0, 64),), -0.2, 0.2)), 0.05, 1.0)
    out_grad = bell_draw(key_of[3], (TOKENS, D), 0.1, 0.59765625, ((0, 64),))
    w_gate = bell_draw(key_of[4], (EXPERTS, D, FF), (D // 2) ** -0.5, 0.1875, ((0, 64), (2, 4)))
    w_up = bell_draw(key_of[5], (EXPERTS, D, FF), (D // 2) ** -0.5, 0.1875, ((0, 64), (2, 4)))
    w_down = bell_draw(key_of[6], (EXPERTS, FF, D), FF ** -0.5, 0.1875, ((0, 64), (1, 4)))
    return dict(tokens=tokens, routes=routes, gate_weights=gate_weights, out_grad=out_grad, w_gate=w_gate, w_up=w_up, w_down=w_down)


clamp_limit = 7.0
sigmoid_slope = 1.702


def unit_backward(gate_pre, up_pre, hidden_grad):
    glu = jnp.minimum(gate_pre, clamp_limit)
    linear = jnp.clip(up_pre, -clamp_limit, clamp_limit)
    sigma = jax.nn.sigmoid(sigmoid_slope * glu)
    active = glu * sigma
    hidden = (active * (linear + 1.0)).astype(jnp.bfloat16)
    slope_term = sigma + sigmoid_slope * active * (1.0 - sigma)
    gate_pre_grad = jnp.where(gate_pre < clamp_limit, hidden_grad * (linear + 1.0) * slope_term, 0.0).astype(jnp.bfloat16)
    up_pre_grad = jnp.where(jnp.abs(up_pre) < clamp_limit, hidden_grad * active, 0.0).astype(jnp.bfloat16)
    return hidden, gate_pre_grad, up_pre_grad


def block_round_total(partial_value):
    rounded = lax.optimization_barrier(partial_value.astype(jnp.bfloat16))
    return jnp.sum(rounded.astype(jnp.float32), axis=0)


def reference(tokens, routes, gate_weights, out_grad, w_gate, w_up, w_down):
    blocks = routes.reshape(N_EP, TOK_DEV * TOPK)
    onehot = (blocks[:, :, None] == jnp.arange(EXPERTS, dtype=jnp.int32)[None, None, :]).astype(jnp.int32)
    slot_rank = jnp.sum((jnp.cumsum(onehot, axis=1) - onehot) * onehot, axis=2)
    source = jnp.arange(N_EP, dtype=jnp.int32)[:, None]
    target = (blocks * (N_EP * CAP) + source * CAP + slot_rank).reshape(-1)
    pair_index = jnp.arange(TOKENS * TOPK, dtype=jnp.int32)
    pair_table = jnp.zeros((EXPERTS * N_EP * CAP,), jnp.int32).at[target].set(pair_index)
    filled = jnp.zeros((EXPERTS * N_EP * CAP,), jnp.int32).at[target].set(1)
    flat_weights = gate_weights.reshape(-1)
    row_count = N_EP * CAP

    def per_expert(running, expert):
        token_acc, gate_acc = running
        slot_pairs = lax.dynamic_slice_in_dim(pair_table, expert * row_count, row_count)
        is_live = lax.dynamic_slice_in_dim(filled, expert * row_count, row_count)[:, None] > 0
        token_index = slot_pairs // TOPK
        x_rows = jnp.where(is_live, tokens[token_index], jnp.zeros((), jnp.bfloat16))
        dy_rows = out_grad[token_index]
        scaled = jnp.where(is_live, flat_weights[slot_pairs][:, None] * dy_rows.astype(jnp.float32), 0.0).astype(jnp.bfloat16)
        gate_mat = w_gate[expert]
        up_mat = w_up[expert]
        down_mat = w_down[expert]
        gate_pre = jnp.dot(x_rows, gate_mat, preferred_element_type=jnp.float32)
        up_pre = jnp.dot(x_rows, up_mat, preferred_element_type=jnp.float32)
        hidden_grad = jnp.dot(scaled, down_mat.T, preferred_element_type=jnp.float32)
        hidden, gate_pre_grad, up_pre_grad = unit_backward(gate_pre, up_pre, hidden_grad)
        unit_block = FF // N_TP
        gate_blocks = gate_pre_grad.astype(jnp.float32).reshape(row_count, N_TP, unit_block)
        up_blocks = up_pre_grad.astype(jnp.float32).reshape(row_count, N_TP, unit_block)
        hidden_blocks = hidden.astype(jnp.float32).reshape(row_count, N_TP, unit_block)
        gate_mat_blocks = gate_mat.astype(jnp.float32).reshape(D, N_TP, unit_block)
        up_mat_blocks = up_mat.astype(jnp.float32).reshape(D, N_TP, unit_block)
        down_blocks = down_mat.astype(jnp.float32).reshape(N_TP, unit_block, D)
        row_partial = jnp.einsum('rnf,dnf->nrd', gate_blocks, gate_mat_blocks) + jnp.einsum('rnf,dnf->nrd', up_blocks, up_mat_blocks)
        row_grad = block_round_total(row_partial).astype(jnp.bfloat16)
        expert_out = block_round_total(jnp.einsum('rnf,nfd->nrd', hidden_blocks, down_blocks))
        token_acc = token_acc.at[token_index].add(jnp.where(is_live, row_grad.astype(jnp.float32), 0.0))
        products = jnp.sum(dy_rows.astype(jnp.float32) * expert_out, axis=1)
        gate_acc = gate_acc.at[slot_pairs].add(jnp.where(is_live[:, 0], products, 0.0))
        gate_weight_grad = jnp.dot(x_rows.T, gate_pre_grad, preferred_element_type=jnp.float32)
        up_weight_grad = jnp.dot(x_rows.T, up_pre_grad, preferred_element_type=jnp.float32)
        down_weight_grad = jnp.dot(hidden.T, scaled, preferred_element_type=jnp.float32)
        return (token_acc, gate_acc), (gate_weight_grad, up_weight_grad, down_weight_grad)

    start = (jnp.zeros((TOKENS, D), jnp.float32), jnp.zeros((TOKENS * TOPK,), jnp.float32))
    (token_acc, gate_acc), grads = lax.scan(per_expert, start, jnp.arange(EXPERTS, dtype=jnp.int32))
    return (token_acc.astype(jnp.bfloat16), gate_acc.reshape(TOKENS, TOPK), grads[0], grads[1], grads[2])
```

```python
import functools

import jax
import jax.numpy as jnp
from jax import lax
from jax.experimental import pallas as pl
from jax.experimental.pallas import tpu as pltpu
from jax.sharding import PartitionSpec as P

MESH = pl.DeviceIdType.MESH
BF16, F32 = jnp.bfloat16, jnp.float32
HIGH = lax.Precision.HIGHEST

CORES = 2
CHIPS_X = 4
MAIN = 16
REST = 4
SLOPE = 1.702
LIMIT = 7.0
AHEAD = 3


def nt(a, b, precision=None):
    return lax.dot_general(a, b, (((1,), (1,)), ((), ())), precision=precision, preferred_element_type=F32)


def tn(a, b, precision=None):
    return lax.dot_general(a, b, (((0,), (0,)), ((), ())), precision=precision, preferred_element_type=F32)


def nn(a, b, precision=None):
    return lax.dot_general(a, b, (((1,), (0,)), ((), ())), precision=precision, preferred_element_type=F32)


def iota(shape, dim):
    return lax.broadcasted_iota(jnp.int32, shape, dim)


def ranks(routes, lanes):
    tokens = routes.shape[0]
    expert = iota((tokens, lanes), 1)
    named = jnp.zeros((tokens, lanes), F32)
    for k in range(routes.shape[1]):
        named = named + jnp.where(routes[:, k : k + 1] == expert, 1.0, 0.0)
    earlier = jnp.where(iota((tokens, tokens), 0) >= iota((tokens, tokens), 1), 1.0, 0.0).astype(BF16)
    upto = nn(earlier, named.astype(BF16))
    return upto * named


def dispatch_kernel(experts, tp_ref, routes_ref, weights_ref, tokens_ref, grads_ref, s_ref):
    routes = routes_ref[...]
    weights = weights_ref[...]
    count = routes.shape[0]
    lanes = max(128, experts)
    expert = iota((count, lanes), 1)
    rank = ranks(routes, lanes)
    weight = jnp.zeros((count, lanes), F32)
    for k in range(routes.shape[1]):
        weight = weight + jnp.where(routes[:, k : k + 1] == expert, weights[:, k : k + 1], 0.0)
    rank_t = rank.T
    weight_t = weight.T
    x = tokens_ref[...]
    dy = grads_ref[...]
    width = x.shape[1]
    piece = width // 2
    some = min(16, experts)
    rows = some * MAIN
    for first in range(0, experts, some):
        rk = jnp.broadcast_to(rank_t[first : first + some][:, None, :], (some, MAIN, count)).reshape(rows, count)
        wt = jnp.broadcast_to(weight_t[first : first + some][:, None, :], (some, MAIN, count)).reshape(rows, count)
        row = (iota((rows, count), 0) & (MAIN - 1)).astype(F32)
        pick = rk == row + 1.0
        hot = jnp.where(pick, 1.0, 0.0).astype(BF16)
        scale = jnp.sum(jnp.where(pick, wt, 0.0), axis=1, keepdims=True)
        at = pl.ds(first * MAIN, rows)
        s_ref[at, 0:width] = nn(hot, x).astype(BF16)
        s_ref[at, width : 2 * width] = (nn(hot, dy) * scale).astype(BF16)
        sub = (iota((rows, count), 0) & (REST - 1)).astype(F32)
        pick = rk == sub + (1.0 + MAIN)
        hot = jnp.where(pick, 1.0, 0.0).astype(BF16)
        scale = jnp.sum(jnp.where(pick, wt, 0.0), axis=1, keepdims=True)
        which = (iota((rows, piece), 0) & (MAIN - 1)) // REST
        out = jnp.where(
            which < 2,
            jnp.where(which == 0, nn(hot, x[:, :piece]), nn(hot, x[:, piece:])),
            jnp.where(which == 2, nn(hot, dy[:, :piece]), nn(hot, dy[:, piece:])) * scale,
        )
        s_ref[at, 2 * width : 2 * width + piece] = out.astype(BF16)


def combine_kernel(experts, routes_ref, weights_ref, bk_ref, q_ref, grad_ref, gate_ref):
    routes = routes_ref[...]
    weights = weights_ref[...]
    count = routes.shape[0]
    lanes = max(128, experts)
    rank = ranks(routes, lanes)
    slots = experts * MAIN
    spread = jnp.where(iota((lanes, slots), 1) // MAIN == iota((lanes, slots), 0), 1.0, 0.0).astype(BF16)
    rk = nn(rank.astype(BF16), spread)
    lane = iota((count, slots), 1) & (MAIN - 1)
    width = bk_ref.shape[1] * 4 // 5
    piece = width // REST
    hot = jnp.where(rk == lane.astype(F32) + 1.0, 1.0, 0.0).astype(BF16)
    total = nn(hot, bk_ref[:, 0:width])
    late = rk == (lane & (REST - 1)).astype(F32) + (1.0 + MAIN)
    for q in range(REST):
        hot = jnp.where(late & (lane // REST == q), 1.0, 0.0).astype(BF16)
        at = slice(q * piece, (q + 1) * piece)
        grad_ref[:, at] = (total[:, at] + nn(hot, bk_ref[:, width : width + piece])).astype(BF16)
    expert = iota((count, lanes), 1)
    products = q_ref[...]
    for k in range(routes.shape[1]):
        mine = routes[:, k : k + 1] == expert
        hot = jnp.where(mine, 1.0, 0.0)
        slot = jnp.sum(jnp.where(mine, rank, 0.0), axis=1, keepdims=True)
        found = nn(hot[:, :experts], products, HIGH)
        chosen = jnp.where(iota(found.shape, 1).astype(F32) + 1.0 == slot, found, 0.0)
        gate_ref[:, k : k + 1] = jnp.sum(chosen, axis=1, keepdims=True) / weights[:, k : k + 1]


def exchange_kernel(
    nz, nj, ny,
    s, wg, wu, wd,
    bk_out, q_out, dwg, dwu, dwd,
    m, xa, da, ga, ua, ha, rt, ra, rb, rc, bo, pq, bk, qin, qy,
    ep_send, ep_recv, y_send, y_recv, f_send, f_recv, ra_send, ra_recv, rb_send, rb_recv, back_send, back_recv,
    q_send, q_recv, qy_send, qy_recv,
):
    nx = nj // CORES
    me = lax.axis_index("ep")
    y = lax.axis_index("tp")
    z, j = lax.div(me, nj), lax.rem(me, nj)
    x, core = lax.div(j, CORES), lax.rem(j, CORES)
    right, left, far = lax.rem(y + 1, ny), lax.rem(y + ny - 1, ny), lax.rem(y + 2, ny)
    width = rt.shape[-1]
    piece = width // 2
    back_piece = width // REST
    main = nj * MAIN
    rest = nj * REST
    rows = main + rest
    half = rows // 2
    half_main = main // 2
    groups = nz

    def remote(src, dst, send, recv, ep, tp):
        return pltpu.make_async_remote_copy(
            src_ref=src, dst_ref=dst, send_sem=send, recv_sem=recv, device_id=(ep, tp), device_id_type=MESH
        )

    def await_bytes(ref, sem):
        pltpu.make_async_copy(ref, ref, sem).wait()

    barrier = pltpu.get_barrier_semaphore()

    def greet(e, _):
        @pl.when(e != me)
        def _():
            pl.semaphore_signal(barrier, inc=1, device_id=(e, y), device_id_type=MESH)

        return 0

    lax.fori_loop(0, nz * nj, greet, 0)
    for other in (right, left, far):
        pl.semaphore_signal(barrier, inc=1, device_id=(me, other), device_id_type=MESH)
    pl.semaphore_wait(barrier, nz * nj - 1 + 3)

    def step_of(g):
        odd, half_g = lax.rem(g, 2), lax.div(g + 1, 2)
        return lax.rem(odd * half_g + (1 - odd) * (nz - half_g), nz)

    def other_j(o):
        return lax.rem(x + o // CORES, nx) * CORES + lax.rem(core + o % CORES, CORES)

    def tile(e):
        return pl.ds(pl.multiple_of(e * MAIN, MAIN), MAIN)

    def send_group(g, orders):
        zd = lax.rem(z + step_of(g), nz)
        for o in orders:
            dest = zd * nj + other_j(o)
            remote(s.at[tile(dest), :], m.at[g, y, tile(j), :], ep_send, ep_recv.at[g], dest, y).start()

    send_group(jnp.int32(0), range(1, nj))
    for g in range(1, min(AHEAD, groups)):
        send_group(jnp.int32(g), range(nj))
    m[0, y, tile(j), :] = s[tile(me), :]

    a, b = iota((main, main), 0), iota((main, main), 1)
    q_of, src_of, j_of = lax.div(a, rest), lax.div(lax.rem(a, rest), REST), lax.rem(a, REST)
    apart = jnp.where(b == src_of * MAIN + q_of * REST + j_of, 1.0, 0.0).astype(BF16)
    q_in, src_in, j_in = lax.div(b, rest), lax.div(lax.rem(b, rest), REST), lax.rem(b, REST)
    together = jnp.where(a == src_in * MAIN + q_in * REST + j_in, 1.0, 0.0).astype(BF16)
    r, lane = iota((rows, 128), 0), iota((rows, 128), 1)
    slot_of = jnp.where(r < main, lax.rem(r, MAIN), MAIN + lax.rem(r, REST))
    at_slot = lane == slot_of
    rr = iota((nj, rows), 1)
    from_src = jnp.where(rr < main, lax.div(rr, MAIN), lax.div(rr - main, REST)) == iota((nj, rows), 0)
    from_src = jnp.where(from_src, 1.0, 0.0)

    def arrive(g):
        @pl.when(g == 0)
        def _():
            await_bytes(m.at[0, y, pl.ds(0, main - MAIN), :], ep_recv.at[0])

        @pl.when(g > 0)
        def _():
            await_bytes(m.at[g, y], ep_recv.at[g])

        remote(m.at[g, y], m.at[g, y], y_send, y_recv.at[0, g], me, right).start()
        remote(m.at[g, y], m.at[g, y], y_send, y_recv.at[1, g], me, left).start()

    def forward(g):
        await_bytes(m.at[g, left], y_recv.at[0, g])
        low = m.at[g, left, pl.ds(0, half_main), :]
        remote(low, low, f_send, f_recv.at[0, g], me, right).start()
        await_bytes(m.at[g, right], y_recv.at[1, g])
        high = m.at[g, right, pl.ds(half_main, half_main), :]
        remote(high, high, f_send, f_recv.at[1, g], me, left).start()

    def compute(g):
        await_bytes(m.at[g, far, pl.ds(0, half_main), :], f_recv.at[0, g])
        await_bytes(m.at[g, far, pl.ds(half_main, half_main), :], f_recv.at[1, g])
        row0 = pl.multiple_of(g * rows, REST * nj)
        at_main, at_rest, at_all = pl.ds(row0, main), pl.ds(row0 + main, rest), pl.ds(row0, rows)
        for slab in range(ny):
            c0 = slab * width
            xa[at_main, c0 : c0 + width] = m[g, slab, :, 0:width]
            da[at_main, c0 : c0 + width] = m[g, slab, :, width : 2 * width]
            pieces = nn(apart, m[g, slab, :, 2 * width : 2 * width + piece]).astype(BF16)
            xa[at_rest, c0 : c0 + piece] = pieces[0:rest]
            xa[at_rest, c0 + piece : c0 + width] = pieces[rest : 2 * rest]
            da[at_rest, c0 : c0 + piece] = pieces[2 * rest : 3 * rest]
            da[at_rest, c0 + piece : c0 + width] = pieces[3 * rest : 4 * rest]
        gate_pre = nn(xa[at_all, :], wg[...])
        up_pre = nn(xa[at_all, :], wu[...])
        hidden_grad = nt(da[at_all, :], wd[...])
        glu = jnp.minimum(gate_pre, LIMIT)
        linear = jnp.clip(up_pre, -LIMIT, LIMIT)
        sigma = jax.nn.sigmoid(SLOPE * glu)
        active = glu * sigma
        hidden = (active * (linear + 1.0)).astype(BF16)
        slope = sigma + SLOPE * active * (1.0 - sigma)
        gpg = jnp.where(gate_pre < LIMIT, hidden_grad * (linear + 1.0) * slope, 0.0).astype(BF16)
        upg = jnp.where(jnp.abs(up_pre) < LIMIT, hidden_grad * active, 0.0).astype(BF16)
        ga[at_all, :] = gpg
        ua[at_all, :] = upg
        ha[at_all, :] = hidden
        for slab in range(ny):
            c0 = slab * width
            term = nt(gpg, wg[c0 : c0 + width, :]) + nt(upg, wu[c0 : c0 + width, :])
            rt[g, slab] = term.astype(BF16)
        low, high = pl.ds(0, half), pl.ds(half, half)
        remote(rt.at[g, far, low], ra.at[g, 0], ra_send, ra_recv.at[0, g], me, right).start()
        remote(rt.at[g, far, high], ra.at[g, 1], ra_send, ra_recv.at[1, g], me, left).start()
        remote(rt.at[g, right, high], rb.at[g, 0, high], rb_send, rb_recv.at[0, g], me, right).start()
        remote(rt.at[g, left, low], rb.at[g, 1, low], rb_send, rb_recv.at[1, g], me, left).start()
        product = jnp.sum(hidden.astype(F32) * hidden_grad, axis=1, keepdims=True)
        laid = nn(from_src, jnp.where(at_slot, product, 0.0), HIGH)
        for src in range(nj):
            pq[g, src] = laid[src : src + 1, :]
        zs = lax.rem(z - step_of(g) + nz, nz)
        for o in range(nj):
            to = other_j(o)

            def send_products(to=to):
                remote(pq.at[g, to], qin.at[me], q_send, q_recv, zs * nj + to, y).start()

            if o == 0:
                pl.when(g > 0)(send_products)
            else:
                send_products()

    def partly(g):
        low, high = pl.ds(0, half), pl.ds(half, half)
        await_bytes(ra.at[g, 0], ra_recv.at[0, g])
        rc[g, 0] = (ra[g, 0].astype(F32) + rt[g, right, low].astype(F32)).astype(BF16)
        remote(rc.at[g, 0], rb.at[g, 0, low], rb_send, rb_recv.at[0, g], me, right).start()
        await_bytes(ra.at[g, 1], ra_recv.at[1, g])
        rc[g, 1] = (ra[g, 1].astype(F32) + rt[g, left, high].astype(F32)).astype(BF16)
        remote(rc.at[g, 1], rb.at[g, 1, high], rb_send, rb_recv.at[1, g], me, left).start()

    def give_back(g):
        await_bytes(rb.at[g, 0], rb_recv.at[0, g])
        await_bytes(rb.at[g, 1], rb_recv.at[1, g])
        total = rt[g, y].astype(F32) + rb[g, 0].astype(F32) + rb[g, 1].astype(F32)
        done = total.astype(BF16)
        bo[g, :, 0:width] = done[0:main]
        stacked = jnp.concatenate(
            [done[main:rows, q * back_piece : (q + 1) * back_piece] for q in range(REST)], axis=0
        )
        bo[g, :, width : width + back_piece] = nn(together, stacked).astype(BF16)
        zs = lax.rem(z - step_of(g) + nz, nz)
        for o in range(nj):
            to = other_j(o)

            def send_rows(to=to):
                remote(bo.at[g, tile(to), :], bk.at[tile(me), :], back_send, back_recv, zs * nj + to, y).start()

            if o == 0:
                pl.when(g > 0)(send_rows)
            else:
                send_rows()

    def step(i, _):
        @pl.when(i + AHEAD < groups)
        def _():
            send_group(i + AHEAD, range(nj))

        pl.when(i < groups)(lambda: arrive(i))
        pl.when((i >= 1) & (i < groups + 1))(lambda: forward(i - 1))
        pl.when((i >= 2) & (i < groups + 2))(lambda: compute(i - 2))
        pl.when((i >= 3) & (i < groups + 3))(lambda: partly(i - 3))
        pl.when(i >= 4)(lambda: give_back(i - 4))
        return 0

    lax.fori_loop(0, groups + 4, step, 0)

    bk[tile(me), :] = bo[0, tile(j), :]
    qin[me] = pq[0, j]
    await_bytes(qin.at[pl.ds(0, nz * nj - 1)], q_recv)
    remote(qin, qy.at[0], qy_send.at[0], qy_recv.at[0], me, right).start()
    remote(qin, qy.at[1], qy_send.at[1], qy_recv.at[1], me, left).start()
    remote(qin, qy.at[2], qy_send.at[2], qy_recv.at[2], me, far).start()

    block = min(256, xa.shape[1])

    def weight_grads(i, _):
        at = pl.ds(pl.multiple_of(i * block, block), block)
        dwg[at, :] = tn(xa[:, at], ga[...])
        dwu[at, :] = tn(xa[:, at], ua[...])
        dwd[:, at] = tn(ha[...], da[:, at])
        return 0

    lax.fori_loop(0, xa.shape[1] // block, weight_grads, 0)

    await_bytes(bk.at[pl.ds(0, (nz * nj - 1) * MAIN), :], back_recv)
    bk_out[...] = bk[...]
    for k in range(3):
        await_bytes(qy.at[k], qy_recv.at[k])
        await_bytes(qin, qy_send.at[k])
    q_out[...] = qin[...] + qy[0] + qy[1] + qy[2]

    everything = pl.ds(0, (nz * nj - 1) * MAIN)
    await_bytes(s.at[everything, :], ep_send)
    for _ in range(2):
        await_bytes(m.at[:, 0], y_send)
        await_bytes(m.at[:, 0, pl.ds(0, half_main), :], f_send)
        await_bytes(ra.at[:, 0], ra_send)
        await_bytes(rb.at[:, 0], rb_send)
    await_bytes(bk.at[everything, :], back_send)
    await_bytes(qin.at[pl.ds(0, nz * nj - 1)], q_send)


def local(nz, nj, ny, tokens, routes, gate_weights, out_grad, w_gate, w_up, w_down):
    count, model = tokens.shape
    units = w_gate.shape[2]
    top = routes.shape[1]
    experts = nz * nj
    width = model // ny
    wide, back_wide = width * 5 // 2, width * 5 // 4
    vmem = pl.BlockSpec(memory_space=pltpu.VMEM)
    tp = lax.axis_index("tp").reshape(1)
    sent = pl.pallas_call(
        functools.partial(dispatch_kernel, experts),
        out_shape=jax.ShapeDtypeStruct((experts * MAIN, wide), BF16),
        grid_spec=pltpu.PrefetchScalarGridSpec(
            num_scalar_prefetch=1,
            grid=(1,),
            in_specs=[
                pl.BlockSpec((count, top), lambda i, t: (0, 0)),
                pl.BlockSpec((count, top), lambda i, t: (0, 0)),
                pl.BlockSpec((count, width), lambda i, t: (0, t[0])),
                pl.BlockSpec((count, width), lambda i, t: (0, t[0])),
            ],
            out_specs=pl.BlockSpec((experts * MAIN, wide), lambda i, t: (0, 0)),
        ),
        compiler_params=pltpu.CompilerParams(vmem_limit_bytes=40 << 20),
        name="dispatch",
    )(tp, routes, gate_weights, tokens, out_grad)

    groups, main, rows = nz, nj * MAIN, nj * (MAIN + REST)
    all_rows = groups * rows
    dma = pltpu.SemaphoreType.DMA
    back, products, dwg, dwu, dwd = pl.pallas_call(
        functools.partial(exchange_kernel, nz, nj, ny),
        out_shape=(
            jax.ShapeDtypeStruct((experts * MAIN, back_wide), BF16),
            jax.ShapeDtypeStruct((experts, 1, 128), F32),
            jax.ShapeDtypeStruct((model, units), F32),
            jax.ShapeDtypeStruct((model, units), F32),
            jax.ShapeDtypeStruct((units, model), F32),
        ),
        in_specs=[vmem] * 4,
        out_specs=(vmem,) * 5,
        scratch_shapes=[
            pltpu.VMEM((groups, ny, main, wide), BF16),
            pltpu.VMEM((all_rows, model), BF16),
            pltpu.VMEM((all_rows, model), BF16),
            pltpu.VMEM((all_rows, units), BF16),
            pltpu.VMEM((all_rows, units), BF16),
            pltpu.VMEM((all_rows, units), BF16),
            pltpu.VMEM((groups, ny, rows, width), BF16),
            pltpu.VMEM((groups, 2, rows // 2, width), BF16),
            pltpu.VMEM((groups, 2, rows, width), BF16),
            pltpu.VMEM((groups, 2, rows // 2, width), BF16),
            pltpu.VMEM((groups, main, back_wide), BF16),
            pltpu.VMEM((groups, nj, 1, 128), F32),
            pltpu.VMEM((experts * MAIN, back_wide), BF16),
            pltpu.VMEM((experts, 1, 128), F32),
            pltpu.VMEM((3, experts, 1, 128), F32),
            dma, dma((groups,)),
            dma, dma((2, groups)),
            dma, dma((2, groups)),
            dma, dma((2, groups)),
            dma, dma((2, groups)),
            dma, dma,
            dma, dma,
            dma((3,)), dma((3,)),
        ],
        compiler_params=pltpu.CompilerParams(
            collective_id=0, has_side_effects=True, vmem_limit_bytes=63 << 20
        ),
        name="exchange",
    )(sent, w_gate[0], w_up[0], w_down[0])

    token_grad, gate_grad = pl.pallas_call(
        functools.partial(combine_kernel, experts),
        out_shape=(
            jax.ShapeDtypeStruct((count, width), BF16),
            jax.ShapeDtypeStruct((count, top), F32),
        ),
        in_specs=[vmem] * 4,
        out_specs=(vmem, vmem),
        compiler_params=pltpu.CompilerParams(vmem_limit_bytes=40 << 20),
        name="combine",
    )(routes, gate_weights, back, products.reshape(experts, 128))
    return token_grad, gate_grad, dwg[None], dwu[None], dwd[None]


def solution(mesh):
    nj = CHIPS_X * CORES
    nz, ny = mesh.shape["ep"] // nj, mesh.shape["tp"]
    in_specs = (
        P("ep", None),
        P("ep", None),
        P("ep", None),
        P("ep", None),
        P("ep", None, "tp"),
        P("ep", None, "tp"),
        P("ep", "tp", None),
    )
    out_specs = (P("ep", "tp"), P("ep", None), P("ep", None, "tp"), P("ep", None, "tp"), P("ep", "tp", None))
    return jax.shard_map(
        functools.partial(local, nz, nj, ny), mesh=mesh, in_specs=in_specs, out_specs=out_specs, check_vma=False
    )
```

```python
import functools

import jax
import jax.numpy as jnp
from jax import lax
from jax.experimental import pallas as pl
from jax.experimental.pallas import tpu as pltpu
from jax.sharding import PartitionSpec as P

MESH = pl.DeviceIdType.MESH
BF16, F32 = jnp.bfloat16, jnp.float32
HIGH = lax.Precision.HIGHEST

CORES = 2
CHIPS_X = 4
MAIN = 16
REST = 4
SLOPE = 1.702
LIMIT = 7.0
DISTANCE = (0, 2, -2, 1, -1, 3, -3, 4)
NEAR = (3, 4)


def nt(a, b, precision=None):
    return lax.dot_general(a, b, (((1,), (1,)), ((), ())), precision=precision, preferred_element_type=F32)


def tn(a, b, precision=None):
    return lax.dot_general(a, b, (((0,), (0,)), ((), ())), precision=precision, preferred_element_type=F32)


def nn(a, b, precision=None):
    return lax.dot_general(a, b, (((1,), (0,)), ((), ())), precision=precision, preferred_element_type=F32)


def iota(shape, dim):
    return lax.broadcasted_iota(jnp.int32, shape, dim)


def ranks(routes, experts):
    top, tokens = routes.shape
    expert = iota((experts, tokens), 0)
    named = jnp.zeros((experts, tokens), F32)
    for k in range(top):
        named = named + jnp.where(routes[k : k + 1, :] == expert, 1.0, 0.0)
    earlier = jnp.where(iota((tokens, tokens), 0) <= iota((tokens, tokens), 1), 1.0, 0.0).astype(BF16)
    return nn(named.astype(BF16), earlier) * named


def exchange_kernel(
    nz, nj, ny,
    routes, weights, tokens, grads, wg_hbm, wu_hbm, wd_hbm,
    bk, q_out, dwg_hbm, dwu_hbm, dwd_hbm,
    x_in, dy_in, wg, wu, wd, rank, weight, s, s_near, s_here, m, xa, da, ga, ua, ha, rt, ra, rb, rc, bo, pq, qin, qy,
    dwg, dwu, dwd,
    in_sem, w_sem, own_sem, dw_sem,
    ep_send, ep_recv, near_send, near_recv, y_send, y_recv, f_send, f_recv, ra_send, ra_recv, rb_send, rb_recv,
    back_send, back_recv, q_send, q_recv, qy_send, qy_recv,
):
    nx = nj // CORES
    experts = nz * nj
    me = lax.axis_index("ep")
    y = lax.axis_index("tp")
    z, j = lax.div(me, nj), lax.rem(me, nj)
    x, core = lax.div(j, CORES), lax.rem(j, CORES)
    right, left, far = lax.rem(y + 1, ny), lax.rem(y + ny - 1, ny), lax.rem(y + 2, ny)
    width = rt.shape[-1]
    piece = width // REST
    packed = width + piece
    main = nj * MAIN
    rest = nj * REST
    rows = main + rest
    half = rows // 2
    half_main = main // 2
    groups = nz
    count = x_in.shape[0]

    def remote(src, dst, send, recv, ep, tp):
        return pltpu.make_async_remote_copy(
            src_ref=src, dst_ref=dst, send_sem=send, recv_sem=recv, device_id=(ep, tp), device_id_type=MESH
        )

    def await_bytes(ref, sem):
        pltpu.make_async_copy(ref, ref, sem).wait()

    loads = [pltpu.make_async_copy(a, b, in_sem.at[k]) for k, (a, b) in enumerate(((tokens, x_in), (grads, dy_in)))]
    loads += [
        pltpu.make_async_copy(a, b, w_sem.at[k]) for k, (a, b) in enumerate(((wg_hbm, wg), (wu_hbm, wu), (wd_hbm, wd)))
    ]
    for load in loads:
        load.start()

    barrier = pltpu.get_barrier_semaphore()

    def greet(e, _):
        @pl.when(e != me)
        def _():
            pl.semaphore_signal(barrier, inc=1, device_id=(e, y), device_id_type=MESH)

        return 0

    lax.fori_loop(0, experts, greet, 0)
    for other in (right, left, far):
        pl.semaphore_signal(barrier, inc=1, device_id=(me, other), device_id_type=MESH)

    distances = sum((d % nz) << (4 * k) for k, d in enumerate(DISTANCE[:groups]))

    def step_of(g):
        if isinstance(g, int):
            return DISTANCE[g] % nz
        return lax.rem(lax.shift_right_logical(jnp.int32(distances), 4 * g), 16)

    def other_j(o):
        return lax.rem(x + o // CORES, nx) * CORES + lax.rem(core + o % CORES, CORES)

    def tile(e):
        return pl.ds(pl.multiple_of(e * MAIN, MAIN), MAIN)

    rank[...] = ranks(routes[...], experts)
    expert = iota((experts, count), 0)
    weight_of = jnp.zeros((experts, count), F32)
    for k in range(routes.shape[0]):
        weight_of = weight_of + jnp.where(routes[k : k + 1, :] == expert, weights[k : k + 1, :], 0.0)
    weight[...] = weight_of
    loads[0].wait()
    loads[1].wait()

    row = iota((main, count), 0)
    quarter = lax.div(lax.rem(iota((main, piece), 0), MAIN), REST)
    own_columns = pl.ds(pl.multiple_of(y * width, width), width)

    def pickers(g):
        zd = lax.rem(z + step_of(g), nz)
        at = pl.ds(pl.multiple_of(zd * nj, nj), nj)
        rk = jnp.broadcast_to(rank[at, :][:, None, :], (nj, MAIN, count)).reshape(main, count)
        wt = jnp.broadcast_to(weight[at, :][:, None, :], (nj, MAIN, count)).reshape(main, count)
        out = []
        for slot in (lax.rem(row, MAIN) + 1, lax.rem(row, REST) + 1 + MAIN):
            pick = rk == slot.astype(F32)
            hot = jnp.where(pick, 1.0, 0.0).astype(BF16)
            out.append((hot, jnp.sum(jnp.where(pick, wt, 0.0), axis=1, keepdims=True)))
        return out

    def pack(out, values, picks, scaled):
        (hot, scale), (hot_rest, scale_rest) = picks
        body = nn(hot, values)
        tail = nn(hot_rest, values)
        edge = tail[:, 0:piece]
        for q in range(1, REST):
            edge = jnp.where(quarter == q, tail[:, q * piece : (q + 1) * piece], edge)
        if scaled:
            body, edge = body * scale, edge * scale_rest
        out[:, 0:width] = body.astype(BF16)
        out[:, width:packed] = edge.astype(BF16)

    def pack_own(g, _):
        picks = pickers(g)
        pack(s.at[g, 0], x_in[:, own_columns], picks, False)
        pack(s.at[g, 1], dy_in[:, own_columns], picks, True)
        return 0

    def send_own(g):
        zd = lax.rem(z + step_of(g), nz)
        for o in range(nj):
            to = other_j(o)
            dest = zd * nj + to
            if g in NEAR:
                src, dst = s.at[g, 1, tile(to), :], m.at[g, y, 1, tile(j), :]
            else:
                src, dst = s.at[g, :, tile(to), :], m.at[g, y, :, tile(j), :]
            remote(src, dst, ep_send, ep_recv.at[g], dest, y).start()

    lax.fori_loop(1, groups, pack_own, 0)
    pl.semaphore_wait(barrier, experts - 1 + 3)
    for g in (3, 4, 1, 2):
        send_own(g)

    picks = pickers(0)
    for slab in range(ny):
        pack(s_here.at[slab, 0], x_in[:, slab * width : (slab + 1) * width], picks, False)
        pack(s_here.at[slab, 1], dy_in[:, slab * width : (slab + 1) * width], picks, True)
    for o in range(1, nj):
        to = other_j(o)
        remote(
            s_here.at[:, :, tile(to), :], m.at[0, :, :, tile(j), :], ep_send, ep_recv.at[0], z * nj + to, y
        ).start()
    for slab in range(ny):
        for k in range(2):
            m[0, slab, k, tile(j), :] = s_here[slab, k, tile(j), :]
    for g in (5, 6):
        send_own(g)
    for n, g in enumerate(NEAR):
        picks = pickers(g)
        for slab in range(ny):
            pack(s_near.at[n, slab], x_in[:, slab * width : (slab + 1) * width], picks, False)
        zd = lax.rem(z + step_of(g), nz)
        for o in range(nj):
            to = other_j(o)
            remote(
                s_near.at[n, :, tile(to), :], m.at[g, :, 0, tile(j), :], near_send, near_recv.at[n], zd * nj + to, y
            ).start()
    send_own(7)

    a, b = iota((main, main), 0), iota((main, main), 1)
    q_of, src_of, j_of = lax.div(a, rest), lax.div(lax.rem(a, rest), REST), lax.rem(a, REST)
    apart = jnp.where(b == src_of * MAIN + q_of * REST + j_of, 1.0, 0.0).astype(BF16)
    q_in, src_in, j_in = lax.div(b, rest), lax.div(lax.rem(b, rest), REST), lax.rem(b, REST)
    together = jnp.where(a == src_in * MAIN + q_in * REST + j_in, 1.0, 0.0).astype(BF16)
    r, lane = iota((rows, 128), 0), iota((rows, 128), 1)
    slot_of = jnp.where(r < main, lax.rem(r, MAIN), MAIN + lax.rem(r, REST))
    at_slot = lane == slot_of
    rr = iota((nj, rows), 1)
    from_src = jnp.where(rr < main, lax.div(rr, MAIN), lax.div(rr - main, REST)) == iota((nj, rows), 0)
    from_src = jnp.where(from_src, 1.0, 0.0)

    def part(g, slab):
        return m.at[g, slab, 1] if g in NEAR else m.at[g, slab]

    def halves(g, slab):
        if g in NEAR:
            return [m.at[g, slab, 1, pl.ds(h * half_main, half_main), :] for h in range(2)]
        return [m.at[g, slab, :, pl.ds(h * half_main, half_main), :] for h in range(2)]

    def arrive(g):
        await_bytes(part(g, y), ep_recv.at[g])
        remote(part(g, y), part(g, y), y_send, y_recv.at[0, g], me, right).start()
        remote(part(g, y), part(g, y), y_send, y_recv.at[1, g], me, left).start()

    def forward(g):
        await_bytes(part(g, left), y_recv.at[0, g])
        low = halves(g, left)[0]
        remote(low, low, f_send, f_recv.at[0, g], me, right).start()
        await_bytes(part(g, right), y_recv.at[1, g])
        high = halves(g, right)[1]
        remote(high, high, f_send, f_recv.at[1, g], me, left).start()

    def gathered(g):
        @pl.when(g == 0)
        def _():
            await_bytes(m.at[0, :, :, pl.ds(0, main - MAIN), :], ep_recv.at[0])
            for load in loads[2:]:
                load.wait()

        for n, near in enumerate(NEAR):

            @pl.when(g == near)
            def _(n=n, near=near):
                await_bytes(m.at[near, :, 0], near_recv.at[n])
                for h in range(2):
                    await_bytes(halves(near, far)[h], f_recv.at[h, near])

        @pl.when((g != 0) & (g != NEAR[0]) & (g != NEAR[1]))
        def _():
            for h in range(2):
                await_bytes(m.at[g, far, :, pl.ds(h * half_main, half_main), :], f_recv.at[h, g])

    def compute(g):
        gathered(g)
        row0 = pl.multiple_of(g * rows, REST * nj)
        at_main, at_rest, at_all = pl.ds(row0, main), pl.ds(row0 + main, rest), pl.ds(row0, rows)
        for slab in range(ny):
            c0 = slab * width
            for k, out in enumerate((xa, da)):
                out[at_main, c0 : c0 + width] = m[g, slab, k, :, 0:width]
                pieces = nn(apart, m[g, slab, k, :, width:packed]).astype(BF16)
                for q in range(REST):
                    out[at_rest, c0 + q * piece : c0 + (q + 1) * piece] = pieces[q * rest : (q + 1) * rest]
        gate_pre = nn(xa[at_all, :], wg[...])
        up_pre = nn(xa[at_all, :], wu[...])
        hidden_grad = nt(da[at_all, :], wd[...])
        glu = jnp.minimum(gate_pre, LIMIT)
        linear = jnp.clip(up_pre, -LIMIT, LIMIT)
        sigma = jax.nn.sigmoid(SLOPE * glu)
        active = glu * sigma
        hidden = (active * (linear + 1.0)).astype(BF16)
        slope = sigma + SLOPE * active * (1.0 - sigma)
        gpg = jnp.where(gate_pre < LIMIT, hidden_grad * (linear + 1.0) * slope, 0.0).astype(BF16)
        upg = jnp.where(jnp.abs(up_pre) < LIMIT, hidden_grad * active, 0.0).astype(BF16)
        ga[at_all, :] = gpg
        ua[at_all, :] = upg
        ha[at_all, :] = hidden
        for slab in range(ny):
            c0 = slab * width
            term = nt(gpg, wg[c0 : c0 + width, :]) + nt(upg, wu[c0 : c0 + width, :])
            rt[g, slab] = term.astype(BF16)
        low, high = pl.ds(0, half), pl.ds(half, half)
        remote(rt.at[g, far, low], ra.at[g, 0], ra_send, ra_recv.at[0, g], me, right).start()
        remote(rt.at[g, far, high], ra.at[g, 1], ra_send, ra_recv.at[1, g], me, left).start()
        remote(rt.at[g, right, high], rb.at[g, 0, high], rb_send, rb_recv.at[0, g], me, right).start()
        remote(rt.at[g, left, low], rb.at[g, 1, low], rb_send, rb_recv.at[1, g], me, left).start()
        product = jnp.sum(hidden.astype(F32) * hidden_grad, axis=1, keepdims=True)
        laid = nn(from_src, jnp.where(at_slot, product, 0.0), HIGH)
        for src in range(nj):
            pq[g, src] = laid[src : src + 1, :]
        zs = lax.rem(z - step_of(g) + nz, nz)
        for o in range(nj):
            to = other_j(o)

            def send_products(to=to):
                remote(pq.at[g, to], qin.at[me], q_send, q_recv, zs * nj + to, y).start()

            if o == 0:
                pl.when(g > 0)(send_products)
            else:
                send_products()

    def partly(g):
        low, high = pl.ds(0, half), pl.ds(half, half)
        await_bytes(ra.at[g, 0], ra_recv.at[0, g])
        rc[g, 0] = (ra[g, 0].astype(F32) + rt[g, right, low].astype(F32)).astype(BF16)
        remote(rc.at[g, 0], rb.at[g, 0, low], rb_send, rb_recv.at[0, g], me, right).start()
        await_bytes(ra.at[g, 1], ra_recv.at[1, g])
        rc[g, 1] = (ra[g, 1].astype(F32) + rt[g, left, high].astype(F32)).astype(BF16)
        remote(rc.at[g, 1], rb.at[g, 1, high], rb_send, rb_recv.at[1, g], me, left).start()

    def give_back(g):
        await_bytes(rb.at[g, 0], rb_recv.at[0, g])
        await_bytes(rb.at[g, 1], rb_recv.at[1, g])
        total = rt[g, y].astype(F32) + rb[g, 0].astype(F32) + rb[g, 1].astype(F32)
        done = total.astype(BF16)
        bo[g, :, 0:width] = done[0:main]
        stacked = jnp.concatenate([done[main:rows, q * piece : (q + 1) * piece] for q in range(REST)], axis=0)
        bo[g, :, width:packed] = nn(together, stacked).astype(BF16)
        zs = lax.rem(z - step_of(g) + nz, nz)
        for o in range(nj):
            to = other_j(o)

            def send_rows(to=to):
                remote(bo.at[g, tile(to), :], bk.at[tile(me), :], back_send, back_recv, zs * nj + to, y).start()

            if o == 0:
                pl.when(g > 0)(send_rows)
            else:
                send_rows()

    def step(i, _):
        @pl.when(i == 0)
        def _():
            arrive(3)
            arrive(4)
            forward(3)
            forward(4)

        @pl.when(i == 1)
        def _():
            arrive(1)
            arrive(2)

        pl.when(i == 5)(lambda: arrive(7))
        pl.when((i >= 1) & (i < groups + 1))(lambda: partly(i - 1))

        @pl.when(i == 1)
        def _():
            forward(1)
            forward(2)
            arrive(5)
            arrive(6)

        pl.when(i == 2)(lambda: forward(5))
        pl.when(i == 3)(lambda: forward(6))
        pl.when(i == 6)(lambda: forward(7))
        pl.when(i >= 2)(lambda: give_back(i - 2))
        pl.when(i < groups)(lambda: compute(i))
        return 0

    lax.fori_loop(0, groups + 2, step, 0)

    own_copy = pltpu.make_async_copy(bo.at[0, tile(j), :], bk.at[tile(me), :], own_sem)
    own_copy.start()
    qin[me] = pq[0, j]
    await_bytes(qin.at[pl.ds(0, experts - 1)], q_recv)
    remote(qin, qy.at[0], qy_send.at[0], qy_recv.at[0], me, right).start()
    remote(qin, qy.at[1], qy_send.at[1], qy_recv.at[1], me, left).start()
    remote(qin, qy.at[2], qy_send.at[2], qy_recv.at[2], me, far).start()

    block = min(256, xa.shape[1])

    def weight_grads(i, _):
        at = pl.ds(pl.multiple_of(i * block, block), block)
        dwg[at, :] = tn(xa[:, at], ga[...])
        dwu[at, :] = tn(xa[:, at], ua[...])
        dwd[:, at] = tn(ha[...], da[:, at])
        pltpu.make_async_copy(dwg.at[at, :], dwg_hbm.at[at, :], dw_sem.at[0]).start()
        pltpu.make_async_copy(dwu.at[at, :], dwu_hbm.at[at, :], dw_sem.at[1]).start()
        pltpu.make_async_copy(dwd.at[:, at], dwd_hbm.at[:, at], dw_sem.at[2]).start()
        return 0

    lax.fori_loop(0, xa.shape[1] // block, weight_grads, 0)

    for k in range(3):
        await_bytes(qy.at[k], qy_recv.at[k])
        await_bytes(qin, qy_send.at[k])
    q_out[...] = qin[...] + qy[0] + qy[1] + qy[2]

    await_bytes(m.at[0:2], ep_send)
    await_bytes(m.at[0, 0], ep_send)
    await_bytes(m.at[0, 0, :, 0:half_main, :], ep_send)
    await_bytes(m.at[0:2, :, 0], near_send)
    for _ in range(2):
        await_bytes(m.at[0:5, 0], y_send)
        await_bytes(m.at[0:2, 0, 1], y_send)
        await_bytes(m.at[0:5, 0, :, 0:half_main, :], f_send)
        await_bytes(m.at[0:2, 0, 1, 0:half_main, :], f_send)
        await_bytes(ra.at[:, 0], ra_send)
        await_bytes(rb.at[:, 0], rb_send)
    everything = pl.ds(0, (experts - 1) * MAIN)
    await_bytes(bk.at[everything, :], back_send)
    await_bytes(qin.at[pl.ds(0, experts - 1)], q_send)
    own_copy.wait()
    for k, (a, b) in enumerate(((dwg, dwg_hbm), (dwu, dwu_hbm), (dwd, dwd_hbm))):
        pltpu.make_async_copy(a, b, dw_sem.at[k]).wait()
    await_bytes(bk.at[everything, :], back_recv)


def finish_kernel(
    experts, routes_ref, weights_ref, bk_ref, q_ref, a_in, b_in, c_in,
    grad_ref, gate_ref, a_out, b_out, c_out,
    a, b, c, in_sem, out_sem,
):
    parts = 4
    copies = []
    for n, (src, mid, dst) in enumerate(((a_in, a, a_out), (b_in, b, b_out), (c_in, c, c_out))):
        size = src.shape[0] // parts
        for k in range(parts):
            at = pl.ds(k * size, size)
            first = pltpu.make_async_copy(src.at[at, :], mid.at[at, :], in_sem.at[n, k])
            second = pltpu.make_async_copy(mid.at[at, :], dst.at[at, :], out_sem.at[n, k])
            first.start()
            copies.append((first, second))

    routes = routes_ref[...]
    count = routes.shape[1]
    rank = ranks(routes, experts)
    slots = experts * MAIN
    spread = jnp.where(lax.div(iota((experts, slots), 1), MAIN) == iota((experts, slots), 0), 1.0, 0.0).astype(BF16)
    rk = tn(rank.astype(BF16), spread)
    for first, second in copies[: len(copies) // 2]:
        first.wait()
        second.start()
    lane = lax.rem(iota((count, slots), 1), MAIN)
    width = bk_ref.shape[1] * REST // (REST + 1)
    piece = width // REST
    hot = jnp.where(rk == lane.astype(F32) + 1.0, 1.0, 0.0).astype(BF16)
    total = nn(hot, bk_ref[:, 0:width])
    for first, second in copies[len(copies) // 2 :]:
        first.wait()
        second.start()
    late = rk == lax.rem(lane, REST).astype(F32) + (1.0 + MAIN)
    for q in range(REST):
        hot = jnp.where(late & (lax.div(lane, REST) == q), 1.0, 0.0).astype(BF16)
        at = slice(q * piece, (q + 1) * piece)
        grad_ref[:, at] = (total[:, at] + nn(hot, bk_ref[:, width : width + piece])).astype(BF16)
    products = q_ref[...]
    expert = iota((experts, count), 0)
    for k in range(routes.shape[0]):
        mine = routes[k : k + 1, :] == expert
        slot = jnp.sum(jnp.where(mine, rank, 0.0), axis=0, keepdims=True)
        found = tn(products, jnp.where(mine, 1.0, 0.0), HIGH)
        chosen = jnp.where(iota(found.shape, 0).astype(F32) + 1.0 == slot, found, 0.0)
        gate_ref[k : k + 1, :] = jnp.sum(chosen, axis=0, keepdims=True) / weights_ref[k : k + 1, :]
    for first, second in copies:
        second.wait()


def local(nz, nj, ny, tokens, routes, gate_weights, out_grad, w_gate, w_up, w_down):
    count, model = tokens.shape
    units = w_gate.shape[2]
    top = routes.shape[1]
    experts = nz * nj
    width = model // ny
    packed = width * (REST + 1) // REST
    vmem = pl.BlockSpec(memory_space=pltpu.VMEM)
    hbm = pl.BlockSpec(memory_space=pltpu.HBM)
    routes_t, weights_t = routes.T, gate_weights.T

    groups, main, rows = nz, nj * MAIN, nj * (MAIN + REST)
    all_rows = groups * rows
    dma = pltpu.SemaphoreType.DMA
    weight_shapes = (
        jax.ShapeDtypeStruct((model, units), F32),
        jax.ShapeDtypeStruct((model, units), F32),
        jax.ShapeDtypeStruct((units, model), F32),
    )
    back, products, dwg, dwu, dwd = pl.pallas_call(
        functools.partial(exchange_kernel, nz, nj, ny),
        out_shape=(
            jax.ShapeDtypeStruct((experts * MAIN, packed), BF16),
            jax.ShapeDtypeStruct((experts, 1, 128), F32),
            *weight_shapes,
        ),
        in_specs=[vmem, vmem] + [hbm] * 5,
        out_specs=(hbm, vmem, hbm, hbm, hbm),
        scratch_shapes=[
            pltpu.VMEM((count, model), BF16),
            pltpu.VMEM((count, model), BF16),
            pltpu.VMEM((model, units), BF16),
            pltpu.VMEM((model, units), BF16),
            pltpu.VMEM((units, model), BF16),
            pltpu.VMEM((experts, count), F32),
            pltpu.VMEM((experts, count), F32),
            pltpu.VMEM((groups, 2, main, packed), BF16),
            pltpu.VMEM((len(NEAR), ny, main, packed), BF16),
            pltpu.VMEM((ny, 2, main, packed), BF16),
            pltpu.VMEM((groups, ny, 2, main, packed), BF16),
            pltpu.VMEM((all_rows, model), BF16),
            pltpu.VMEM((all_rows, model), BF16),
            pltpu.VMEM((all_rows, units), BF16),
            pltpu.VMEM((all_rows, units), BF16),
            pltpu.VMEM((all_rows, units), BF16),
            pltpu.VMEM((groups, ny, rows, width), BF16),
            pltpu.VMEM((groups, 2, rows // 2, width), BF16),
            pltpu.VMEM((groups, 2, rows, width), BF16),
            pltpu.VMEM((groups, 2, rows // 2, width), BF16),
            pltpu.VMEM((groups, main, packed), BF16),
            pltpu.VMEM((groups, nj, 1, 128), F32),
            pltpu.VMEM((experts, 1, 128), F32),
            pltpu.VMEM((3, experts, 1, 128), F32),
            *(pltpu.VMEM(w.shape, F32) for w in weight_shapes),
            dma((2,)), dma((3,)), dma, dma((3,)),
            dma, dma((groups,)),
            dma, dma((len(NEAR),)),
            dma, dma((2, groups)),
            dma, dma((2, groups)),
            dma, dma((2, groups)),
            dma, dma((2, groups)),
            dma, dma,
            dma, dma,
            dma((3,)), dma((3,)),
        ],
        compiler_params=pltpu.CompilerParams(
            collective_id=0, has_side_effects=True, vmem_limit_bytes=67_043_328
        ),
        name="exchange",
    )(routes_t, weights_t, tokens, out_grad, w_gate[0], w_up[0], w_down[0])

    token_grad, gate_grad, dwg, dwu, dwd = pl.pallas_call(
        functools.partial(finish_kernel, experts),
        out_shape=(
            jax.ShapeDtypeStruct((count, width), BF16),
            jax.ShapeDtypeStruct((top, count), F32),
            *weight_shapes,
        ),
        in_specs=[vmem] * 4 + [hbm] * 3,
        out_specs=(vmem, vmem, hbm, hbm, hbm),
        scratch_shapes=[*(pltpu.VMEM(w.shape, F32) for w in weight_shapes), dma((3, 4)), dma((3, 4))],
        compiler_params=pltpu.CompilerParams(vmem_limit_bytes=67_043_328),
        name="finish",
    )(routes_t, weights_t, back, products.reshape(experts, 128), dwg, dwu, dwd)
    return token_grad, gate_grad.T, dwg[None], dwu[None], dwd[None]


def solution(mesh):
    nj = CHIPS_X * CORES
    nz, ny = mesh.shape["ep"] // nj, mesh.shape["tp"]
    in_specs = (
        P("ep", None),
        P("ep", None),
        P("ep", None),
        P("ep", None),
        P("ep", None, "tp"),
        P("ep", None, "tp"),
        P("ep", "tp", None),
    )
    out_specs = (P("ep", "tp"), P("ep", None), P("ep", None, "tp"), P("ep", None, "tp"), P("ep", "tp", None))
    return jax.shard_map(
        functools.partial(local, nz, nj, ny), mesh=mesh, in_specs=in_specs, out_specs=out_specs, check_vma=False
    )
```

```python
import functools

import jax
import jax.numpy as jnp
from jax import lax
from jax.experimental import pallas as pl
from jax.experimental.pallas import tpu as pltpu
from jax.sharding import PartitionSpec as P

MESH = pl.DeviceIdType.MESH
BF16, F32 = jnp.bfloat16, jnp.float32
HIGH = lax.Precision.HIGHEST

CORES = 2
CHIPS_X = 4
MAIN = 16
REST = 4
SLOPE = 1.702
LIMIT = 7.0
DISTANCE = (0, 2, -2, 3, -3, 4, 1, -1)
NEAR = (6, 7)


def nt(a, b, precision=None):
    return lax.dot_general(a, b, (((1,), (1,)), ((), ())), precision=precision, preferred_element_type=F32)


def tn(a, b, precision=None):
    return lax.dot_general(a, b, (((0,), (0,)), ((), ())), precision=precision, preferred_element_type=F32)


def nn(a, b, precision=None):
    return lax.dot_general(a, b, (((1,), (0,)), ((), ())), precision=precision, preferred_element_type=F32)


def iota(shape, dim):
    return lax.broadcasted_iota(jnp.int32, shape, dim)


def ranks(routes, experts):
    top, tokens = routes.shape
    expert = iota((experts, tokens), 0)
    named = jnp.zeros((experts, tokens), F32)
    for k in range(top):
        named = named + jnp.where(routes[k : k + 1, :] == expert, 1.0, 0.0)
    earlier = jnp.where(iota((tokens, tokens), 0) <= iota((tokens, tokens), 1), 1.0, 0.0).astype(BF16)
    return nn(named.astype(BF16), earlier) * named


def exchange_kernel(
    nz, nj, ny,
    routes, weights, tokens, grads, wg_hbm, wu_hbm, wd_hbm,
    bk, q_out, dwg_hbm, dwu_hbm, dwd_hbm,
    x_in, dy_in, wg, wu, wd, rank, weight, s, s_near, s_here, m, xa, da, ga, ua, ha, rt, ra, rb, rc, bo, pq, qin, qy,
    dwg, dwu, dwd,
    in_sem, w_sem, own_sem, dw_sem,
    ep_send, ep_recv, near_send, near_recv, y_send, y_recv, f_send, f_recv, ra_send, ra_recv, rb_send, rb_recv,
    back_send, back_recv, q_send, q_recv, qy_send, qy_recv,
):
    nx = nj // CORES
    experts = nz * nj
    me = lax.axis_index("ep")
    y = lax.axis_index("tp")
    z, j = lax.div(me, nj), lax.rem(me, nj)
    x, core = lax.div(j, CORES), lax.rem(j, CORES)
    right, left, far = lax.rem(y + 1, ny), lax.rem(y + ny - 1, ny), lax.rem(y + 2, ny)
    width = rt.shape[-1]
    piece = width // REST
    packed = width + piece
    main = nj * MAIN
    rest = nj * REST
    rows = main + rest
    half = rows // 2
    half_main = main // 2
    groups = nz
    count = x_in.shape[0]

    def remote(src, dst, send, recv, ep, tp):
        return pltpu.make_async_remote_copy(
            src_ref=src, dst_ref=dst, send_sem=send, recv_sem=recv, device_id=(ep, tp), device_id_type=MESH
        )

    def await_bytes(ref, sem):
        pltpu.make_async_copy(ref, ref, sem).wait()

    loads = [pltpu.make_async_copy(a, b, in_sem.at[k]) for k, (a, b) in enumerate(((tokens, x_in), (grads, dy_in)))]
    loads += [
        pltpu.make_async_copy(a, b, w_sem.at[k]) for k, (a, b) in enumerate(((wg_hbm, wg), (wu_hbm, wu), (wd_hbm, wd)))
    ]
    for load in loads:
        load.start()

    barrier = pltpu.get_barrier_semaphore()

    def greet(e, _):
        @pl.when(e != me)
        def _():
            pl.semaphore_signal(barrier, inc=1, device_id=(e, y), device_id_type=MESH)

        return 0

    lax.fori_loop(0, experts, greet, 0)
    for other in (right, left, far):
        pl.semaphore_signal(barrier, inc=1, device_id=(me, other), device_id_type=MESH)

    distances = sum((d % nz) << (4 * k) for k, d in enumerate(DISTANCE[:groups]))

    def step_of(g):
        if isinstance(g, int):
            return DISTANCE[g] % nz
        return lax.rem(lax.shift_right_logical(jnp.int32(distances), 4 * g), 16)

    def other_j(o):
        return lax.rem(x + o // CORES, nx) * CORES + lax.rem(core + o % CORES, CORES)

    def tile(e):
        return pl.ds(pl.multiple_of(e * MAIN, MAIN), MAIN)

    rank[...] = ranks(routes[...], experts)
    expert = iota((experts, count), 0)
    weight_of = jnp.zeros((experts, count), F32)
    for k in range(routes.shape[0]):
        weight_of = weight_of + jnp.where(routes[k : k + 1, :] == expert, weights[k : k + 1, :], 0.0)
    weight[...] = weight_of
    loads[0].wait()
    loads[1].wait()

    row = iota((main, count), 0)
    quarter = lax.div(lax.rem(iota((main, piece), 0), MAIN), REST)
    own_columns = pl.ds(pl.multiple_of(y * width, width), width)

    def pickers(g):
        zd = lax.rem(z + step_of(g), nz)
        at = pl.ds(pl.multiple_of(zd * nj, nj), nj)
        rk = jnp.broadcast_to(rank[at, :][:, None, :], (nj, MAIN, count)).reshape(main, count)
        wt = jnp.broadcast_to(weight[at, :][:, None, :], (nj, MAIN, count)).reshape(main, count)
        out = []
        for slot in (lax.rem(row, MAIN) + 1, lax.rem(row, REST) + 1 + MAIN):
            pick = rk == slot.astype(F32)
            hot = jnp.where(pick, 1.0, 0.0).astype(BF16)
            out.append((hot, jnp.sum(jnp.where(pick, wt, 0.0), axis=1, keepdims=True)))
        return out

    def pack(out, values, picks, scaled):
        (hot, scale), (hot_rest, scale_rest) = picks
        body = nn(hot, values)
        tail = nn(hot_rest, values)
        edge = tail[:, 0:piece]
        for q in range(1, REST):
            edge = jnp.where(quarter == q, tail[:, q * piece : (q + 1) * piece], edge)
        if scaled:
            body, edge = body * scale, edge * scale_rest
        out[:, 0:width] = body.astype(BF16)
        out[:, width:packed] = edge.astype(BF16)

    def pack_own(g, _):
        picks = pickers(g)
        pack(s.at[g, 0], x_in[:, own_columns], picks, False)
        pack(s.at[g, 1], dy_in[:, own_columns], picks, True)
        return 0

    def send_own(g):
        zd = lax.rem(z + step_of(g), nz)
        for o in range(nj):
            to = other_j(o)
            dest = zd * nj + to
            if g in NEAR:
                src, dst = s.at[g, 1, tile(to), :], m.at[g, y, 1, tile(j), :]
            else:
                src, dst = s.at[g, :, tile(to), :], m.at[g, y, :, tile(j), :]
            remote(src, dst, ep_send, ep_recv.at[g], dest, y).start()

    lax.fori_loop(1, groups, pack_own, 0)
    pl.semaphore_wait(barrier, experts - 1 + 3)
    for g in (6, 7, 1, 2):
        send_own(g)

    picks = pickers(0)
    for slab in range(ny):
        pack(s_here.at[slab, 0], x_in[:, slab * width : (slab + 1) * width], picks, False)
        pack(s_here.at[slab, 1], dy_in[:, slab * width : (slab + 1) * width], picks, True)
    for o in range(1, nj):
        to = other_j(o)
        remote(
            s_here.at[:, :, tile(to), :], m.at[0, :, :, tile(j), :], ep_send, ep_recv.at[0], z * nj + to, y
        ).start()
    for slab in range(ny):
        for k in range(2):
            m[0, slab, k, tile(j), :] = s_here[slab, k, tile(j), :]
    for g in (3, 4, 5):
        send_own(g)
    for n, g in enumerate(NEAR):
        picks = pickers(g)
        for slab in range(ny):
            pack(s_near.at[n, slab], x_in[:, slab * width : (slab + 1) * width], picks, False)
        zd = lax.rem(z + step_of(g), nz)
        for o in range(nj):
            to = other_j(o)
            remote(
                s_near.at[n, :, tile(to), :], m.at[g, :, 0, tile(j), :], near_send, near_recv.at[n], zd * nj + to, y
            ).start()

    a, b = iota((main, main), 0), iota((main, main), 1)
    q_of, src_of, j_of = lax.div(a, rest), lax.div(lax.rem(a, rest), REST), lax.rem(a, REST)
    apart = jnp.where(b == src_of * MAIN + q_of * REST + j_of, 1.0, 0.0).astype(BF16)
    q_in, src_in, j_in = lax.div(b, rest), lax.div(lax.rem(b, rest), REST), lax.rem(b, REST)
    together = jnp.where(a == src_in * MAIN + q_in * REST + j_in, 1.0, 0.0).astype(BF16)
    r, lane = iota((rows, 128), 0), iota((rows, 128), 1)
    slot_of = jnp.where(r < main, lax.rem(r, MAIN), MAIN + lax.rem(r, REST))
    at_slot = lane == slot_of
    rr = iota((nj, rows), 1)
    from_src = jnp.where(rr < main, lax.div(rr, MAIN), lax.div(rr - main, REST)) == iota((nj, rows), 0)
    from_src = jnp.where(from_src, 1.0, 0.0)

    def part(g, slab):
        return m.at[g, slab, 1] if g in NEAR else m.at[g, slab]

    def halves(g, slab):
        if g in NEAR:
            return [m.at[g, slab, 1, pl.ds(h * half_main, half_main), :] for h in range(2)]
        return [m.at[g, slab, :, pl.ds(h * half_main, half_main), :] for h in range(2)]

    def arrive(g):
        await_bytes(part(g, y), ep_recv.at[g])
        remote(part(g, y), part(g, y), y_send, y_recv.at[0, g], me, right).start()
        remote(part(g, y), part(g, y), y_send, y_recv.at[1, g], me, left).start()

    def forward(g):
        await_bytes(part(g, left), y_recv.at[0, g])
        low = halves(g, left)[0]
        remote(low, low, f_send, f_recv.at[0, g], me, right).start()
        await_bytes(part(g, right), y_recv.at[1, g])
        high = halves(g, right)[1]
        remote(high, high, f_send, f_recv.at[1, g], me, left).start()

    def gathered(g):
        @pl.when(g == 0)
        def _():
            await_bytes(m.at[0, :, :, pl.ds(0, main - MAIN), :], ep_recv.at[0])
            for load in loads[2:]:
                load.wait()

        for n, near in enumerate(NEAR):

            @pl.when(g == near)
            def _(n=n, near=near):
                await_bytes(m.at[near, :, 0], near_recv.at[n])
                for h in range(2):
                    await_bytes(halves(near, far)[h], f_recv.at[h, near])

        @pl.when((g != 0) & (g != NEAR[0]) & (g != NEAR[1]))
        def _():
            for h in range(2):
                await_bytes(m.at[g, far, :, pl.ds(h * half_main, half_main), :], f_recv.at[h, g])

    def compute(g):
        gathered(g)
        row0 = pl.multiple_of(g * rows, REST * nj)
        at_main, at_rest, at_all = pl.ds(row0, main), pl.ds(row0 + main, rest), pl.ds(row0, rows)
        for slab in range(ny):
            c0 = slab * width
            for k, out in enumerate((xa, da)):
                out[at_main, c0 : c0 + width] = m[g, slab, k, :, 0:width]
                pieces = nn(apart, m[g, slab, k, :, width:packed]).astype(BF16)
                for q in range(REST):
                    out[at_rest, c0 + q * piece : c0 + (q + 1) * piece] = pieces[q * rest : (q + 1) * rest]
        gate_pre = nn(xa[at_all, :], wg[...])
        up_pre = nn(xa[at_all, :], wu[...])
        hidden_grad = nt(da[at_all, :], wd[...])
        glu = jnp.minimum(gate_pre, LIMIT)
        linear = jnp.clip(up_pre, -LIMIT, LIMIT)
        sigma = jax.nn.sigmoid(SLOPE * glu)
        active = glu * sigma
        hidden = (active * (linear + 1.0)).astype(BF16)
        slope = sigma + SLOPE * active * (1.0 - sigma)
        gpg = jnp.where(gate_pre < LIMIT, hidden_grad * (linear + 1.0) * slope, 0.0).astype(BF16)
        upg = jnp.where(jnp.abs(up_pre) < LIMIT, hidden_grad * active, 0.0).astype(BF16)
        ga[at_all, :] = gpg
        ua[at_all, :] = upg
        ha[at_all, :] = hidden
        for slab in range(ny):
            c0 = slab * width
            term = nt(gpg, wg[c0 : c0 + width, :]) + nt(upg, wu[c0 : c0 + width, :])
            rt[g, slab] = term.astype(BF16)
        low, high = pl.ds(0, half), pl.ds(half, half)
        remote(rt.at[g, far, low], ra.at[g, 0], ra_send, ra_recv.at[0, g], me, right).start()
        remote(rt.at[g, far, high], ra.at[g, 1], ra_send, ra_recv.at[1, g], me, left).start()
        remote(rt.at[g, right, high], rb.at[g, 0, high], rb_send, rb_recv.at[0, g], me, right).start()
        remote(rt.at[g, left, low], rb.at[g, 1, low], rb_send, rb_recv.at[1, g], me, left).start()
        product = jnp.sum(hidden.astype(F32) * hidden_grad, axis=1, keepdims=True)
        laid = nn(from_src, jnp.where(at_slot, product, 0.0), HIGH)
        for src in range(nj):
            pq[g, src] = laid[src : src + 1, :]
        zs = lax.rem(z - step_of(g) + nz, nz)
        for o in range(nj):
            to = other_j(o)

            def send_products(to=to):
                remote(pq.at[g, to], qin.at[me], q_send, q_recv, zs * nj + to, y).start()

            if o == 0:
                pl.when(g > 0)(send_products)
            else:
                send_products()

    def partly(g):
        low, high = pl.ds(0, half), pl.ds(half, half)
        await_bytes(ra.at[g, 0], ra_recv.at[0, g])
        rc[g, 0] = (ra[g, 0].astype(F32) + rt[g, right, low].astype(F32)).astype(BF16)
        remote(rc.at[g, 0], rb.at[g, 0, low], rb_send, rb_recv.at[0, g], me, right).start()
        await_bytes(ra.at[g, 1], ra_recv.at[1, g])
        rc[g, 1] = (ra[g, 1].astype(F32) + rt[g, left, high].astype(F32)).astype(BF16)
        remote(rc.at[g, 1], rb.at[g, 1, high], rb_send, rb_recv.at[1, g], me, left).start()

    def give_back(g):
        await_bytes(rb.at[g, 0], rb_recv.at[0, g])
        await_bytes(rb.at[g, 1], rb_recv.at[1, g])
        total = rt[g, y].astype(F32) + rb[g, 0].astype(F32) + rb[g, 1].astype(F32)
        done = total.astype(BF16)
        bo[g, :, 0:width] = done[0:main]
        stacked = jnp.concatenate([done[main:rows, q * piece : (q + 1) * piece] for q in range(REST)], axis=0)
        bo[g, :, width:packed] = nn(together, stacked).astype(BF16)
        zs = lax.rem(z - step_of(g) + nz, nz)
        for o in range(nj):
            to = other_j(o)

            def send_rows(to=to):
                remote(bo.at[g, tile(to), :], bk.at[tile(me), :], back_send, back_recv, zs * nj + to, y).start()

            if o == 0:
                pl.when(g > 0)(send_rows)
            else:
                send_rows()

    block = min(256, xa.shape[1])

    def weight_grads(i, _):
        at = pl.ds(pl.multiple_of(i * block, block), block)
        dwg[at, :] = tn(xa[:, at], ga[...])
        dwu[at, :] = tn(xa[:, at], ua[...])
        dwd[:, at] = tn(ha[...], da[:, at])
        pltpu.make_async_copy(dwg.at[at, :], dwg_hbm.at[at, :], dw_sem.at[0]).start()
        pltpu.make_async_copy(dwu.at[at, :], dwu_hbm.at[at, :], dw_sem.at[1]).start()
        pltpu.make_async_copy(dwd.at[:, at], dwd_hbm.at[:, at], dw_sem.at[2]).start()
        return 0

    def step(i, _):
        @pl.when(i == 0)
        def _():
            arrive(6)
            arrive(7)
            forward(6)
            forward(7)
            arrive(1)
            arrive(2)

        @pl.when(i == 1)
        def _():
            forward(1)
            forward(2)
            arrive(3)
            arrive(4)

        pl.when(i == 2)(lambda: forward(3))
        pl.when(i == 3)(lambda: arrive(5))
        pl.when(i == 4)(lambda: forward(5))
        compute(i)
        pl.when(i == 2)(lambda: forward(4))
        pl.when(i >= 1)(lambda: partly(i - 1))
        pl.when(i >= 2)(lambda: give_back(i - 2))
        return 0

    lax.fori_loop(0, groups, step, 0)
    blocks = xa.shape[1] // block
    cuts = (0, blocks * 3 // 8, blocks * 6 // 8, blocks)
    lax.fori_loop(cuts[0], cuts[1], weight_grads, 0)
    partly(groups - 1)
    give_back(groups - 2)
    lax.fori_loop(cuts[1], cuts[2], weight_grads, 0)
    give_back(groups - 1)

    own_copy = pltpu.make_async_copy(bo.at[0, tile(j), :], bk.at[tile(me), :], own_sem)
    own_copy.start()
    qin[me] = pq[0, j]
    await_bytes(qin.at[pl.ds(0, experts - 1)], q_recv)
    remote(qin, qy.at[0], qy_send.at[0], qy_recv.at[0], me, right).start()
    remote(qin, qy.at[1], qy_send.at[1], qy_recv.at[1], me, left).start()
    remote(qin, qy.at[2], qy_send.at[2], qy_recv.at[2], me, far).start()

    lax.fori_loop(cuts[2], cuts[3], weight_grads, 0)

    for k in range(3):
        await_bytes(qy.at[k], qy_recv.at[k])
        await_bytes(qin, qy_send.at[k])
    q_out[...] = qin[...] + qy[0] + qy[1] + qy[2]

    await_bytes(m.at[0:2], ep_send)
    await_bytes(m.at[0, 0], ep_send)
    await_bytes(m.at[0, 0, :, 0:half_main, :], ep_send)
    await_bytes(m.at[0:2, :, 0], near_send)
    for _ in range(2):
        await_bytes(m.at[0:5, 0], y_send)
        await_bytes(m.at[0:2, 0, 1], y_send)
        await_bytes(m.at[0:5, 0, :, 0:half_main, :], f_send)
        await_bytes(m.at[0:2, 0, 1, 0:half_main, :], f_send)
        await_bytes(ra.at[:, 0], ra_send)
        await_bytes(rb.at[:, 0], rb_send)
    everything = pl.ds(0, (experts - 1) * MAIN)
    await_bytes(bk.at[everything, :], back_send)
    await_bytes(qin.at[pl.ds(0, experts - 1)], q_send)
    own_copy.wait()
    for k, (a, b) in enumerate(((dwg, dwg_hbm), (dwu, dwu_hbm), (dwd, dwd_hbm))):
        pltpu.make_async_copy(a, b, dw_sem.at[k]).wait()
    await_bytes(bk.at[everything, :], back_recv)


def finish_kernel(
    experts, routes_ref, weights_ref, bk_ref, q_ref, a_in, b_in, c_in,
    grad_ref, gate_ref, a_out, b_out, c_out,
    a, b, c, in_sem, out_sem,
):
    parts = 4
    copies = []
    for n, (src, mid, dst) in enumerate(((a_in, a, a_out), (b_in, b, b_out), (c_in, c, c_out))):
        size = src.shape[0] // parts
        for k in range(parts):
            at = pl.ds(k * size, size)
            first = pltpu.make_async_copy(src.at[at, :], mid.at[at, :], in_sem.at[n, k])
            second = pltpu.make_async_copy(mid.at[at, :], dst.at[at, :], out_sem.at[n, k])
            first.start()
            copies.append((first, second))

    routes = routes_ref[...]
    count = routes.shape[1]
    rank = ranks(routes, experts)
    slots = experts * MAIN
    spread = jnp.where(lax.div(iota((experts, slots), 1), MAIN) == iota((experts, slots), 0), 1.0, 0.0).astype(BF16)
    rk = tn(rank.astype(BF16), spread)
    for first, second in copies[: len(copies) // 2]:
        first.wait()
        second.start()
    lane = lax.rem(iota((count, slots), 1), MAIN)
    width = bk_ref.shape[1] * REST // (REST + 1)
    piece = width // REST
    hot = jnp.where(rk == lane.astype(F32) + 1.0, 1.0, 0.0).astype(BF16)
    total = nn(hot, bk_ref[:, 0:width])
    for first, second in copies[len(copies) // 2 :]:
        first.wait()
        second.start()
    late = rk == lax.rem(lane, REST).astype(F32) + (1.0 + MAIN)
    for q in range(REST):
        hot = jnp.where(late & (lax.div(lane, REST) == q), 1.0, 0.0).astype(BF16)
        at = slice(q * piece, (q + 1) * piece)
        grad_ref[:, at] = (total[:, at] + nn(hot, bk_ref[:, width : width + piece])).astype(BF16)
    products = q_ref[...]
    expert = iota((experts, count), 0)
    for k in range(routes.shape[0]):
        mine = routes[k : k + 1, :] == expert
        slot = jnp.sum(jnp.where(mine, rank, 0.0), axis=0, keepdims=True)
        found = tn(products, jnp.where(mine, 1.0, 0.0), HIGH)
        chosen = jnp.where(iota(found.shape, 0).astype(F32) + 1.0 == slot, found, 0.0)
        gate_ref[k : k + 1, :] = jnp.sum(chosen, axis=0, keepdims=True) / weights_ref[k : k + 1, :]
    for first, second in copies:
        second.wait()


def local(nz, nj, ny, tokens, routes, gate_weights, out_grad, w_gate, w_up, w_down):
    count, model = tokens.shape
    units = w_gate.shape[2]
    top = routes.shape[1]
    experts = nz * nj
    width = model // ny
    packed = width * (REST + 1) // REST
    vmem = pl.BlockSpec(memory_space=pltpu.VMEM)
    hbm = pl.BlockSpec(memory_space=pltpu.HBM)
    routes_t, weights_t = routes.T, gate_weights.T

    groups, main, rows = nz, nj * MAIN, nj * (MAIN + REST)
    all_rows = groups * rows
    dma = pltpu.SemaphoreType.DMA
    weight_shapes = (
        jax.ShapeDtypeStruct((model, units), F32),
        jax.ShapeDtypeStruct((model, units), F32),
        jax.ShapeDtypeStruct((units, model), F32),
    )
    back, products, dwg, dwu, dwd = pl.pallas_call(
        functools.partial(exchange_kernel, nz, nj, ny),
        out_shape=(
            jax.ShapeDtypeStruct((experts * MAIN, packed), BF16),
            jax.ShapeDtypeStruct((experts, 1, 128), F32),
            *weight_shapes,
        ),
        in_specs=[vmem, vmem] + [hbm] * 5,
        out_specs=(hbm, vmem, hbm, hbm, hbm),
        scratch_shapes=[
            pltpu.VMEM((count, model), BF16),
            pltpu.VMEM((count, model), BF16),
            pltpu.VMEM((model, units), BF16),
            pltpu.VMEM((model, units), BF16),
            pltpu.VMEM((units, model), BF16),
            pltpu.VMEM((experts, count), F32),
            pltpu.VMEM((experts, count), F32),
            pltpu.VMEM((groups, 2, main, packed), BF16),
            pltpu.VMEM((len(NEAR), ny, main, packed), BF16),
            pltpu.VMEM((ny, 2, main, packed), BF16),
            pltpu.VMEM((groups, ny, 2, main, packed), BF16),
            pltpu.VMEM((all_rows, model), BF16),
            pltpu.VMEM((all_rows, model), BF16),
            pltpu.VMEM((all_rows, units), BF16),
            pltpu.VMEM((all_rows, units), BF16),
            pltpu.VMEM((all_rows, units), BF16),
            pltpu.VMEM((groups, ny, rows, width), BF16),
            pltpu.VMEM((groups, 2, rows // 2, width), BF16),
            pltpu.VMEM((groups, 2, rows, width), BF16),
            pltpu.VMEM((groups, 2, rows // 2, width), BF16),
            pltpu.VMEM((groups, main, packed), BF16),
            pltpu.VMEM((groups, nj, 1, 128), F32),
            pltpu.VMEM((experts, 1, 128), F32),
            pltpu.VMEM((3, experts, 1, 128), F32),
            *(pltpu.VMEM(w.shape, F32) for w in weight_shapes),
            dma((2,)), dma((3,)), dma, dma((3,)),
            dma, dma((groups,)),
            dma, dma((len(NEAR),)),
            dma, dma((2, groups)),
            dma, dma((2, groups)),
            dma, dma((2, groups)),
            dma, dma((2, groups)),
            dma, dma,
            dma, dma,
            dma((3,)), dma((3,)),
        ],
        compiler_params=pltpu.CompilerParams(
            collective_id=0, has_side_effects=True, vmem_limit_bytes=67_043_328
        ),
        name="exchange",
    )(routes_t, weights_t, tokens, out_grad, w_gate[0], w_up[0], w_down[0])

    token_grad, gate_grad, dwg, dwu, dwd = pl.pallas_call(
        functools.partial(finish_kernel, experts),
        out_shape=(
            jax.ShapeDtypeStruct((count, width), BF16),
            jax.ShapeDtypeStruct((top, count), F32),
            *weight_shapes,
        ),
        in_specs=[vmem] * 4 + [hbm] * 3,
        out_specs=(vmem, vmem, hbm, hbm, hbm),
        scratch_shapes=[*(pltpu.VMEM(w.shape, F32) for w in weight_shapes), dma((3, 4)), dma((3, 4))],
        compiler_params=pltpu.CompilerParams(vmem_limit_bytes=67_043_328),
        name="finish",
    )(routes_t, weights_t, back, products.reshape(experts, 128), dwg, dwu, dwd)
    return token_grad, gate_grad.T, dwg[None], dwu[None], dwd[None]


def solution(mesh):
    nj = CHIPS_X * CORES
    nz, ny = mesh.shape["ep"] // nj, mesh.shape["tp"]
    in_specs = (
        P("ep", None),
        P("ep", None),
        P("ep", None),
        P("ep", None),
        P("ep", None, "tp"),
        P("ep", None, "tp"),
        P("ep", "tp", None),
    )
    out_specs = (P("ep", "tp"), P("ep", None), P("ep", None, "tp"), P("ep", None, "tp"), P("ep", "tp", None))
    return jax.shard_map(
        functools.partial(local, nz, nj, ny), mesh=mesh, in_specs=in_specs, out_specs=out_specs, check_vma=False
    )
```

```python
import functools

import jax
import jax.numpy as jnp
from jax import lax
from jax.experimental import pallas as pl
from jax.experimental.pallas import tpu as pltpu
from jax.sharding import PartitionSpec as P

MESH = pl.DeviceIdType.MESH
BF16, F32 = jnp.bfloat16, jnp.float32
HIGH = lax.Precision.HIGHEST

CORES = 2
CHIPS_X = 4
MAIN = 16
REST = 4
SPLIT = 384
SLOPE = 1.702
LIMIT = 7.0
DISTANCE = (0, 2, -2, 3, -3, 4, 1, -1)
NEAR = (6, 7)


def nt(a, b, precision=None):
    return lax.dot_general(a, b, (((1,), (1,)), ((), ())), precision=precision, preferred_element_type=F32)


def tn(a, b, precision=None):
    return lax.dot_general(a, b, (((0,), (0,)), ((), ())), precision=precision, preferred_element_type=F32)


def nn(a, b, precision=None):
    return lax.dot_general(a, b, (((1,), (0,)), ((), ())), precision=precision, preferred_element_type=F32)


def iota(shape, dim):
    return lax.broadcasted_iota(jnp.int32, shape, dim)


def ranks(routes, experts):
    top, tokens = routes.shape
    expert = iota((experts, tokens), 0)
    named = jnp.zeros((experts, tokens), F32)
    for k in range(top):
        named = named + jnp.where(routes[k : k + 1, :] == expert, 1.0, 0.0)
    earlier = jnp.where(iota((tokens, tokens), 0) <= iota((tokens, tokens), 1), 1.0, 0.0).astype(BF16)
    return nn(named.astype(BF16), earlier) * named


def exchange_kernel(
    nz, nj, ny,
    routes, weights, tokens, grads, wg_hbm, wu_hbm, wd_hbm,
    bk, q_out, dwg_hbm, dwu_hbm, dwd_hbm,
    x_in, dy_in, wg, wu, wd, rank, weight, s, s_near, s_edge, s_here, m, xa, da, ga, ua, ha, rt, ra, rb, rc, bo, pq, qin, qy,
    dwg, dwu, dwd,
    in_sem, w_sem, own_sem, dw_sem,
    ep_send, ep_recv, near_send, near_recv, y_send, y_recv, f_send, f_recv, ra_send, ra_recv, rb_send, rb_recv,
    back_send, back_recv, q_send, q_recv, qy_send, qy_recv,
):
    nx = nj // CORES
    experts = nz * nj
    me = lax.axis_index("ep")
    y = lax.axis_index("tp")
    z, j = lax.div(me, nj), lax.rem(me, nj)
    x, core = lax.div(j, CORES), lax.rem(j, CORES)
    right, left, far = lax.rem(y + 1, ny), lax.rem(y + ny - 1, ny), lax.rem(y + 2, ny)
    width = rt.shape[-1]
    piece = width // REST
    packed = width + piece
    main = nj * MAIN
    rest = nj * REST
    rows = main + rest
    half = rows // 2
    half_main = main // 2
    groups = nz
    count = x_in.shape[0]

    def remote(src, dst, send, recv, ep, tp):
        return pltpu.make_async_remote_copy(
            src_ref=src, dst_ref=dst, send_sem=send, recv_sem=recv, device_id=(ep, tp), device_id_type=MESH
        )

    def await_bytes(ref, sem):
        pltpu.make_async_copy(ref, ref, sem).wait()

    loads = [pltpu.make_async_copy(a, b, in_sem.at[k]) for k, (a, b) in enumerate(((tokens, x_in), (grads, dy_in)))]
    loads += [
        pltpu.make_async_copy(a, b, w_sem.at[k]) for k, (a, b) in enumerate(((wg_hbm, wg), (wu_hbm, wu), (wd_hbm, wd)))
    ]
    for load in loads:
        load.start()

    barrier = pltpu.get_barrier_semaphore()

    def greet(e, _):
        @pl.when(e != me)
        def _():
            pl.semaphore_signal(barrier, inc=1, device_id=(e, y), device_id_type=MESH)

        return 0

    lax.fori_loop(0, experts, greet, 0)
    for other in (right, left, far):
        pl.semaphore_signal(barrier, inc=1, device_id=(me, other), device_id_type=MESH)

    distances = sum((d % nz) << (4 * k) for k, d in enumerate(DISTANCE[:groups]))

    def step_of(g):
        if isinstance(g, int):
            return DISTANCE[g] % nz
        return lax.rem(lax.shift_right_logical(jnp.int32(distances), 4 * g), 16)

    def other_j(o):
        return lax.rem(x + o // CORES, nx) * CORES + lax.rem(core + o % CORES, CORES)

    def tile(e):
        return pl.ds(pl.multiple_of(e * MAIN, MAIN), MAIN)

    rank[...] = ranks(routes[...], experts)
    expert = iota((experts, count), 0)
    weight_of = jnp.zeros((experts, count), F32)
    for k in range(routes.shape[0]):
        weight_of = weight_of + jnp.where(routes[k : k + 1, :] == expert, weights[k : k + 1, :], 0.0)
    weight[...] = weight_of
    loads[0].wait()
    loads[1].wait()

    row = iota((main, count), 0)
    quarter = lax.div(lax.rem(iota((main, piece), 0), MAIN), REST)
    own_columns = pl.ds(pl.multiple_of(y * width, width), width)

    def pickers(g):
        zd = lax.rem(z + step_of(g), nz)
        at = pl.ds(pl.multiple_of(zd * nj, nj), nj)
        rk = jnp.broadcast_to(rank[at, :][:, None, :], (nj, MAIN, count)).reshape(main, count)
        wt = jnp.broadcast_to(weight[at, :][:, None, :], (nj, MAIN, count)).reshape(main, count)
        out = []
        for slot in (lax.rem(row, MAIN) + 1, lax.rem(row, REST) + 1 + MAIN):
            pick = rk == slot.astype(F32)
            hot = jnp.where(pick, 1.0, 0.0).astype(BF16)
            out.append((hot, jnp.sum(jnp.where(pick, wt, 0.0), axis=1, keepdims=True)))
        return out

    def pack(out, values, picks, scaled):
        (hot, scale), (hot_rest, scale_rest) = picks
        body = nn(hot, values)
        tail = nn(hot_rest, values)
        edge = tail[:, 0:piece]
        for q in range(1, REST):
            edge = jnp.where(quarter == q, tail[:, q * piece : (q + 1) * piece], edge)
        if scaled:
            body, edge = body * scale, edge * scale_rest
        out[:, 0:width] = body.astype(BF16)
        out[:, width:packed] = edge.astype(BF16)

    def pack_own(g, _):
        picks = pickers(g)
        pack(s.at[g, 0], x_in[:, own_columns], picks, False)
        pack(s.at[g, 1], dy_in[:, own_columns], picks, True)
        return 0

    def send_own(g):
        zd = lax.rem(z + step_of(g), nz)
        for o in range(nj):
            to = other_j(o)
            dest = zd * nj + to
            if g in NEAR:
                src, dst = s.at[g, 1, tile(to), SPLIT:packed], m.at[g, y, 1, tile(j), SPLIT:packed]
            else:
                src, dst = s.at[g, :, tile(to), :], m.at[g, y, :, tile(j), :]
            remote(src, dst, ep_send, ep_recv.at[g], dest, y).start()

    lax.fori_loop(1, groups, pack_own, 0)
    pl.semaphore_wait(barrier, experts - 1 + 3)
    for g in (6, 7, 1, 2):
        send_own(g)

    picks = pickers(0)
    for slab in range(ny):
        pack(s_here.at[slab, 0], x_in[:, slab * width : (slab + 1) * width], picks, False)
        pack(s_here.at[slab, 1], dy_in[:, slab * width : (slab + 1) * width], picks, True)
    for o in range(1, nj):
        to = other_j(o)
        remote(
            s_here.at[:, :, tile(to), :], m.at[0, :, :, tile(j), :], ep_send, ep_recv.at[0], z * nj + to, y
        ).start()
    for slab in range(ny):
        for k in range(2):
            m[0, slab, k, tile(j), :] = s_here[slab, k, tile(j), :]
    for g in (3, 4, 5):
        send_own(g)
    for n, g in enumerate(NEAR):
        picks = pickers(g)
        for slab in range(ny):
            c0 = slab * width
            pack(s_near.at[n, slab], x_in[:, c0 : c0 + width], picks, False)
            hot, scale = picks[0]
            s_edge[n, slab] = (nn(hot, dy_in[:, c0 : c0 + SPLIT]) * scale).astype(BF16)
        zd = lax.rem(z + step_of(g), nz)
        for o in range(nj):
            to = other_j(o)
            dest = zd * nj + to
            src, dst = s_near.at[n, :, tile(to), :], m.at[g, :, 0, tile(j), :]
            remote(src, dst, near_send, near_recv.at[0, n], dest, y).start()
            src, dst = s_edge.at[n, :, tile(to), :], m.at[g, :, 1, tile(j), 0:SPLIT]
            remote(src, dst, near_send, near_recv.at[1, n], dest, y).start()

    a, b = iota((main, main), 0), iota((main, main), 1)
    q_of, src_of, j_of = lax.div(a, rest), lax.div(lax.rem(a, rest), REST), lax.rem(a, REST)
    apart = jnp.where(b == src_of * MAIN + q_of * REST + j_of, 1.0, 0.0).astype(BF16)
    q_in, src_in, j_in = lax.div(b, rest), lax.div(lax.rem(b, rest), REST), lax.rem(b, REST)
    together = jnp.where(a == src_in * MAIN + q_in * REST + j_in, 1.0, 0.0).astype(BF16)
    r, lane = iota((rows, 128), 0), iota((rows, 128), 1)
    slot_of = jnp.where(r < main, lax.rem(r, MAIN), MAIN + lax.rem(r, REST))
    at_slot = lane == slot_of
    rr = iota((nj, rows), 1)
    from_src = jnp.where(rr < main, lax.div(rr, MAIN), lax.div(rr - main, REST)) == iota((nj, rows), 0)
    from_src = jnp.where(from_src, 1.0, 0.0)

    def part(g, slab):
        return m.at[g, slab, 1, :, SPLIT:packed] if g in NEAR else m.at[g, slab]

    def halves(g, slab):
        if g in NEAR:
            return [m.at[g, slab, 1, pl.ds(h * half_main, half_main), SPLIT:packed] for h in range(2)]
        return [m.at[g, slab, :, pl.ds(h * half_main, half_main), :] for h in range(2)]

    def arrive(g):
        await_bytes(part(g, y), ep_recv.at[g])
        remote(part(g, y), part(g, y), y_send, y_recv.at[0, g], me, right).start()
        remote(part(g, y), part(g, y), y_send, y_recv.at[1, g], me, left).start()

    def forward(g):
        await_bytes(part(g, left), y_recv.at[0, g])
        low = halves(g, left)[0]
        remote(low, low, f_send, f_recv.at[0, g], me, right).start()
        await_bytes(part(g, right), y_recv.at[1, g])
        high = halves(g, right)[1]
        remote(high, high, f_send, f_recv.at[1, g], me, left).start()

    def gathered(g):
        @pl.when(g == 0)
        def _():
            await_bytes(m.at[0, :, :, pl.ds(0, main - MAIN), :], ep_recv.at[0])
            for load in loads[2:]:
                load.wait()

        for n, near in enumerate(NEAR):

            @pl.when(g == near)
            def _(n=n, near=near):
                await_bytes(m.at[near, :, 0], near_recv.at[0, n])
                await_bytes(m.at[near, :, 1, :, 0:SPLIT], near_recv.at[1, n])
                for h in range(2):
                    await_bytes(halves(near, far)[h], f_recv.at[h, near])

        @pl.when((g != 0) & (g != NEAR[0]) & (g != NEAR[1]))
        def _():
            for h in range(2):
                await_bytes(m.at[g, far, :, pl.ds(h * half_main, half_main), :], f_recv.at[h, g])

    def compute(g):
        gathered(g)
        row0 = pl.multiple_of(g * rows, REST * nj)
        at_main, at_rest, at_all = pl.ds(row0, main), pl.ds(row0 + main, rest), pl.ds(row0, rows)
        for slab in range(ny):
            c0 = slab * width
            for k, out in enumerate((xa, da)):
                out[at_main, c0 : c0 + width] = m[g, slab, k, :, 0:width]
                pieces = nn(apart, m[g, slab, k, :, width:packed]).astype(BF16)
                for q in range(REST):
                    out[at_rest, c0 + q * piece : c0 + (q + 1) * piece] = pieces[q * rest : (q + 1) * rest]
        gate_pre = nn(xa[at_all, :], wg[...])
        up_pre = nn(xa[at_all, :], wu[...])
        hidden_grad = nt(da[at_all, :], wd[...])
        glu = jnp.minimum(gate_pre, LIMIT)
        linear = jnp.clip(up_pre, -LIMIT, LIMIT)
        sigma = jax.nn.sigmoid(SLOPE * glu)
        active = glu * sigma
        hidden = (active * (linear + 1.0)).astype(BF16)
        slope = sigma + SLOPE * active * (1.0 - sigma)
        gpg = jnp.where(gate_pre < LIMIT, hidden_grad * (linear + 1.0) * slope, 0.0).astype(BF16)
        upg = jnp.where(jnp.abs(up_pre) < LIMIT, hidden_grad * active, 0.0).astype(BF16)
        ga[at_all, :] = gpg
        ua[at_all, :] = upg
        ha[at_all, :] = hidden
        for slab in range(ny):
            c0 = slab * width
            term = nt(gpg, wg[c0 : c0 + width, :]) + nt(upg, wu[c0 : c0 + width, :])
            rt[g, slab] = term.astype(BF16)
        low, high = pl.ds(0, half), pl.ds(half, half)
        remote(rt.at[g, far, low], ra.at[g, 0], ra_send, ra_recv.at[0, g], me, right).start()
        remote(rt.at[g, far, high], ra.at[g, 1], ra_send, ra_recv.at[1, g], me, left).start()
        remote(rt.at[g, right, high], rb.at[g, 0, high], rb_send, rb_recv.at[0, g], me, right).start()
        remote(rt.at[g, left, low], rb.at[g, 1, low], rb_send, rb_recv.at[1, g], me, left).start()
        product = jnp.sum(hidden.astype(F32) * hidden_grad, axis=1, keepdims=True)
        laid = nn(from_src, jnp.where(at_slot, product, 0.0), HIGH)
        for src in range(nj):
            pq[g, src] = laid[src : src + 1, :]
        zs = lax.rem(z - step_of(g) + nz, nz)
        for o in range(nj):
            to = other_j(o)

            def send_products(to=to):
                remote(pq.at[g, to], qin.at[me], q_send, q_recv, zs * nj + to, y).start()

            if o == 0:
                pl.when(g > 0)(send_products)
            else:
                send_products()

    def partly(g):
        low, high = pl.ds(0, half), pl.ds(half, half)
        await_bytes(ra.at[g, 0], ra_recv.at[0, g])
        rc[g, 0] = (ra[g, 0].astype(F32) + rt[g, right, low].astype(F32)).astype(BF16)
        remote(rc.at[g, 0], rb.at[g, 0, low], rb_send, rb_recv.at[0, g], me, right).start()
        await_bytes(ra.at[g, 1], ra_recv.at[1, g])
        rc[g, 1] = (ra[g, 1].astype(F32) + rt[g, left, high].astype(F32)).astype(BF16)
        remote(rc.at[g, 1], rb.at[g, 1, high], rb_send, rb_recv.at[1, g], me, left).start()

    def give_back(g):
        await_bytes(rb.at[g, 0], rb_recv.at[0, g])
        await_bytes(rb.at[g, 1], rb_recv.at[1, g])
        total = rt[g, y].astype(F32) + rb[g, 0].astype(F32) + rb[g, 1].astype(F32)
        done = total.astype(BF16)
        bo[g, :, 0:width] = done[0:main]
        stacked = jnp.concatenate([done[main:rows, q * piece : (q + 1) * piece] for q in range(REST)], axis=0)
        bo[g, :, width:packed] = nn(together, stacked).astype(BF16)
        zs = lax.rem(z - step_of(g) + nz, nz)
        for o in range(nj):
            to = other_j(o)

            def send_rows(to=to):
                remote(bo.at[g, tile(to), :], bk.at[tile(me), :], back_send, back_recv, zs * nj + to, y).start()

            if o == 0:
                pl.when(g > 0)(send_rows)
            else:
                send_rows()

    block = min(256, xa.shape[1])

    def weight_grads(i, _):
        at = pl.ds(pl.multiple_of(i * block, block), block)
        dwg[at, :] = tn(xa[:, at], ga[...])
        dwu[at, :] = tn(xa[:, at], ua[...])
        dwd[:, at] = tn(ha[...], da[:, at])
        pltpu.make_async_copy(dwg.at[at, :], dwg_hbm.at[at, :], dw_sem.at[0]).start()
        pltpu.make_async_copy(dwu.at[at, :], dwu_hbm.at[at, :], dw_sem.at[1]).start()
        pltpu.make_async_copy(dwd.at[:, at], dwd_hbm.at[:, at], dw_sem.at[2]).start()
        return 0

    def step(i, _):
        @pl.when(i == 0)
        def _():
            arrive(6)
            arrive(7)
            forward(6)
            forward(7)
            arrive(1)
            arrive(2)

        @pl.when(i == 1)
        def _():
            forward(1)
            forward(2)
            arrive(3)
            arrive(4)

        pl.when(i == 2)(lambda: forward(3))
        pl.when(i == 3)(lambda: arrive(5))
        pl.when(i == 4)(lambda: forward(5))
        compute(i)
        pl.when(i == 2)(lambda: forward(4))
        pl.when(i >= 1)(lambda: partly(i - 1))
        pl.when(i >= 2)(lambda: give_back(i - 2))
        return 0

    lax.fori_loop(0, groups, step, 0)
    blocks = xa.shape[1] // block
    cuts = (0, blocks * 3 // 8, blocks * 6 // 8, blocks)
    lax.fori_loop(cuts[0], cuts[1], weight_grads, 0)
    partly(groups - 1)
    give_back(groups - 2)
    lax.fori_loop(cuts[1], cuts[2], weight_grads, 0)
    give_back(groups - 1)

    own_copy = pltpu.make_async_copy(bo.at[0, tile(j), :], bk.at[tile(me), :], own_sem)
    own_copy.start()
    qin[me] = pq[0, j]
    await_bytes(qin.at[pl.ds(0, experts - 1)], q_recv)
    remote(qin, qy.at[0], qy_send.at[0], qy_recv.at[0], me, right).start()
    remote(qin, qy.at[1], qy_send.at[1], qy_recv.at[1], me, left).start()
    remote(qin, qy.at[2], qy_send.at[2], qy_recv.at[2], me, far).start()

    lax.fori_loop(cuts[2], cuts[3], weight_grads, 0)

    for k in range(3):
        await_bytes(qy.at[k], qy_recv.at[k])
        await_bytes(qin, qy_send.at[k])
    q_out[...] = qin[...] + qy[0] + qy[1] + qy[2]

    await_bytes(m.at[0:2], ep_send)
    await_bytes(m.at[0, 0, :, 0:half_main, :], ep_send)
    await_bytes(m.at[0, 0:2, 0, :, SPLIT:packed], ep_send)
    await_bytes(m.at[0:2, :, 0], near_send)
    await_bytes(m.at[0:2, :, 1, :, 0:SPLIT], near_send)
    for _ in range(2):
        await_bytes(m.at[0:5, 0], y_send)
        await_bytes(m.at[0:2, 0, 1, :, SPLIT:packed], y_send)
        await_bytes(m.at[0:5, 0, :, 0:half_main, :], f_send)
        await_bytes(m.at[0:2, 0, 1, 0:half_main, SPLIT:packed], f_send)
        await_bytes(ra.at[:, 0], ra_send)
        await_bytes(rb.at[:, 0], rb_send)
    everything = pl.ds(0, (experts - 1) * MAIN)
    await_bytes(bk.at[everything, :], back_send)
    await_bytes(qin.at[pl.ds(0, experts - 1)], q_send)
    own_copy.wait()
    for k, (a, b) in enumerate(((dwg, dwg_hbm), (dwu, dwu_hbm), (dwd, dwd_hbm))):
        pltpu.make_async_copy(a, b, dw_sem.at[k]).wait()
    await_bytes(bk.at[everything, :], back_recv)


def finish_kernel(
    experts, routes_ref, weights_ref, bk_in, q_in, a_in, b_in, c_in,
    grad_ref, gate_ref, a_out, b_out, c_out,
    bk, q, a, b, c, first_sem, in_sem, out_sem,
):
    parts = 4
    load_bk = pltpu.make_async_copy(bk_in, bk, first_sem.at[0])
    load_q = pltpu.make_async_copy(q_in, q, first_sem.at[1])
    load_q.start()
    load_bk.start()
    copies = []
    for n, (src, mid, dst) in enumerate(((a_in, a, a_out), (b_in, b, b_out), (c_in, c, c_out))):
        size = src.shape[0] // parts
        for k in range(parts):
            at = pl.ds(k * size, size)
            first = pltpu.make_async_copy(src.at[at, :], mid.at[at, :], in_sem.at[n, k])
            second = pltpu.make_async_copy(mid.at[at, :], dst.at[at, :], out_sem.at[n, k])
            first.start()
            copies.append((first, second))

    def pass_on(some):
        for first, second in some:
            first.wait()
            second.start()

    routes = routes_ref[...]
    count = routes.shape[1]
    rank = ranks(routes, experts)
    slots = experts * MAIN
    spread = jnp.where(lax.div(iota((experts, slots), 1), MAIN) == iota((experts, slots), 0), 1.0, 0.0).astype(BF16)
    rk = tn(rank.astype(BF16), spread)
    load_q.wait()
    products = q[...]
    expert = iota((experts, count), 0)
    for k in range(routes.shape[0]):
        mine = routes[k : k + 1, :] == expert
        slot = jnp.sum(jnp.where(mine, rank, 0.0), axis=0, keepdims=True)
        found = tn(products, jnp.where(mine, 1.0, 0.0), HIGH)
        chosen = jnp.where(iota(found.shape, 0).astype(F32) + 1.0 == slot, found, 0.0)
        gate_ref[k : k + 1, :] = jnp.sum(chosen, axis=0, keepdims=True) / weights_ref[k : k + 1, :]
    pass_on(copies[:5])
    lane = lax.rem(iota((count, slots), 1), MAIN)
    width = bk.shape[1] * REST // (REST + 1)
    piece = width // REST
    hot = jnp.where(rk == lane.astype(F32) + 1.0, 1.0, 0.0).astype(BF16)
    load_bk.wait()
    total = nn(hot, bk[:, 0:width])
    pass_on(copies[5:9])
    late = rk == lax.rem(lane, REST).astype(F32) + (1.0 + MAIN)
    for n in range(REST):
        hot = jnp.where(late & (lax.div(lane, REST) == n), 1.0, 0.0).astype(BF16)
        at = slice(n * piece, (n + 1) * piece)
        grad_ref[:, at] = (total[:, at] + nn(hot, bk[:, width : width + piece])).astype(BF16)
    pass_on(copies[9:])
    for _, second in copies:
        second.wait()


def local(nz, nj, ny, tokens, routes, gate_weights, out_grad, w_gate, w_up, w_down):
    count, model = tokens.shape
    units = w_gate.shape[2]
    top = routes.shape[1]
    experts = nz * nj
    width = model // ny
    packed = width * (REST + 1) // REST
    vmem = pl.BlockSpec(memory_space=pltpu.VMEM)
    hbm = pl.BlockSpec(memory_space=pltpu.HBM)
    routes_t, weights_t = routes.T, gate_weights.T

    groups, main, rows = nz, nj * MAIN, nj * (MAIN + REST)
    all_rows = groups * rows
    dma = pltpu.SemaphoreType.DMA
    weight_shapes = (
        jax.ShapeDtypeStruct((model, units), F32),
        jax.ShapeDtypeStruct((model, units), F32),
        jax.ShapeDtypeStruct((units, model), F32),
    )
    back, products, dwg, dwu, dwd = pl.pallas_call(
        functools.partial(exchange_kernel, nz, nj, ny),
        out_shape=(
            jax.ShapeDtypeStruct((experts * MAIN, packed), BF16),
            jax.ShapeDtypeStruct((experts, 1, 128), F32),
            *weight_shapes,
        ),
        in_specs=[vmem, vmem] + [hbm] * 5,
        out_specs=(hbm, vmem, hbm, hbm, hbm),
        scratch_shapes=[
            pltpu.VMEM((count, model), BF16),
            pltpu.VMEM((count, model), BF16),
            pltpu.VMEM((model, units), BF16),
            pltpu.VMEM((model, units), BF16),
            pltpu.VMEM((units, model), BF16),
            pltpu.VMEM((experts, count), F32),
            pltpu.VMEM((experts, count), F32),
            pltpu.VMEM((groups, 2, main, packed), BF16),
            pltpu.VMEM((len(NEAR), ny, main, packed), BF16),
            pltpu.VMEM((len(NEAR), ny, main, SPLIT), BF16),
            pltpu.VMEM((ny, 2, main, packed), BF16),
            pltpu.VMEM((groups, ny, 2, main, packed), BF16),
            pltpu.VMEM((all_rows, model), BF16),
            pltpu.VMEM((all_rows, model), BF16),
            pltpu.VMEM((all_rows, units), BF16),
            pltpu.VMEM((all_rows, units), BF16),
            pltpu.VMEM((all_rows, units), BF16),
            pltpu.VMEM((groups, ny, rows, width), BF16),
            pltpu.VMEM((groups, 2, rows // 2, width), BF16),
            pltpu.VMEM((groups, 2, rows, width), BF16),
            pltpu.VMEM((groups, 2, rows // 2, width), BF16),
            pltpu.VMEM((groups, main, packed), BF16),
            pltpu.VMEM((groups, nj, 1, 128), F32),
            pltpu.VMEM((experts, 1, 128), F32),
            pltpu.VMEM((3, experts, 1, 128), F32),
            *(pltpu.VMEM(w.shape, F32) for w in weight_shapes),
            dma((2,)), dma((3,)), dma, dma((3,)),
            dma, dma((groups,)),
            dma, dma((2, len(NEAR))),
            dma, dma((2, groups)),
            dma, dma((2, groups)),
            dma, dma((2, groups)),
            dma, dma((2, groups)),
            dma, dma,
            dma, dma,
            dma((3,)), dma((3,)),
        ],
        compiler_params=pltpu.CompilerParams(
            collective_id=0, has_side_effects=True, vmem_limit_bytes=67_043_328
        ),
        name="exchange",
    )(routes_t, weights_t, tokens, out_grad, w_gate[0], w_up[0], w_down[0])

    token_grad, gate_grad, dwg, dwu, dwd = pl.pallas_call(
        functools.partial(finish_kernel, experts),
        out_shape=(
            jax.ShapeDtypeStruct((count, width), BF16),
            jax.ShapeDtypeStruct((top, count), F32),
            *weight_shapes,
        ),
        in_specs=[vmem] * 2 + [hbm] * 5,
        out_specs=(vmem, vmem, hbm, hbm, hbm),
        scratch_shapes=[
            pltpu.VMEM((experts * MAIN, packed), BF16),
            pltpu.VMEM((experts, 128), F32),
            *(pltpu.VMEM(w.shape, F32) for w in weight_shapes),
            dma((2,)), dma((3, 4)), dma((3, 4)),
        ],
        compiler_params=pltpu.CompilerParams(vmem_limit_bytes=67_043_328),
        name="finish",
    )(routes_t, weights_t, back, products.reshape(experts, 128), dwg, dwu, dwd)
    return token_grad, gate_grad.T, dwg[None], dwu[None], dwd[None]


def solution(mesh):
    nj = CHIPS_X * CORES
    nz, ny = mesh.shape["ep"] // nj, mesh.shape["tp"]
    in_specs = (
        P("ep", None),
        P("ep", None),
        P("ep", None),
        P("ep", None),
        P("ep", None, "tp"),
        P("ep", None, "tp"),
        P("ep", "tp", None),
    )
    out_specs = (P("ep", "tp"), P("ep", None), P("ep", None, "tp"), P("ep", None, "tp"), P("ep", "tp", None))
    return jax.shard_map(
        functools.partial(local, nz, nj, ny), mesh=mesh, in_specs=in_specs, out_specs=out_specs, check_vma=False
    )
```

```python
import functools

import jax
import jax.numpy as jnp
from jax import lax
from jax.experimental import pallas as pl
from jax.experimental.pallas import tpu as pltpu
from jax.sharding import PartitionSpec as P

MESH = pl.DeviceIdType.MESH
BF16, F32 = jnp.bfloat16, jnp.float32
HIGH = lax.Precision.HIGHEST

CORES = 2
CHIPS_X = 4
MAIN = 16
REST = 4
SPLIT = 384
SLOPE = 1.702
LIMIT = 7.0
DISTANCE = (0, 2, -2, 3, -3, 4, 1, -1)
NEAR = (6, 7)


def nt(a, b, precision=None):
    return lax.dot_general(a, b, (((1,), (1,)), ((), ())), precision=precision, preferred_element_type=F32)


def tn(a, b, precision=None):
    return lax.dot_general(a, b, (((0,), (0,)), ((), ())), precision=precision, preferred_element_type=F32)


def nn(a, b, precision=None):
    return lax.dot_general(a, b, (((1,), (0,)), ((), ())), precision=precision, preferred_element_type=F32)


def iota(shape, dim):
    return lax.broadcasted_iota(jnp.int32, shape, dim)


def ranks(routes, experts):
    top, tokens = routes.shape
    expert = iota((experts, tokens), 0)
    named = jnp.zeros((experts, tokens), F32)
    for k in range(top):
        named = named + jnp.where(routes[k : k + 1, :] == expert, 1.0, 0.0)
    earlier = jnp.where(iota((tokens, tokens), 0) <= iota((tokens, tokens), 1), 1.0, 0.0).astype(BF16)
    return nn(named.astype(BF16), earlier) * named


def exchange_kernel(
    nz, nj, ny,
    routes, weights, tokens, grads, wg_hbm, wu_hbm, wd_hbm,
    bk, q_out, dwg_hbm, dwu_hbm, dwd_hbm,
    x_in, dy_in, wg, wu, wd, rank, weight, s, s_near, s_edge, s_here, m, xa, da, ga, ua, ha, rt, ra, rb, rc, bo, pq, qin, qy,
    dwg, dwu, dwd,
    in_sem, w_sem, own_sem, dw_sem,
    ep_send, ep_recv, near_send, near_recv, y_send, y_recv, f_send, f_recv, ra_send, ra_recv, rb_send, rb_recv,
    back_send, back_recv, q_send, q_recv, qy_send, qy_recv,
):
    nx = nj // CORES
    experts = nz * nj
    me = lax.axis_index("ep")
    y = lax.axis_index("tp")
    z, j = lax.div(me, nj), lax.rem(me, nj)
    x, core = lax.div(j, CORES), lax.rem(j, CORES)
    right, left, far = lax.rem(y + 1, ny), lax.rem(y + ny - 1, ny), lax.rem(y + 2, ny)
    width = rt.shape[-1]
    piece = width // REST
    packed = width + piece
    main = nj * MAIN
    rest = nj * REST
    rows = main + rest
    half = rows // 2
    half_main = main // 2
    groups = nz
    count = x_in.shape[0]

    def remote(src, dst, send, recv, ep, tp):
        return pltpu.make_async_remote_copy(
            src_ref=src, dst_ref=dst, send_sem=send, recv_sem=recv, device_id=(ep, tp), device_id_type=MESH
        )

    def await_bytes(ref, sem):
        pltpu.make_async_copy(ref, ref, sem).wait()

    loads = [pltpu.make_async_copy(a, b, in_sem.at[k]) for k, (a, b) in enumerate(((tokens, x_in), (grads, dy_in)))]
    loads += [
        pltpu.make_async_copy(a, b, w_sem.at[k]) for k, (a, b) in enumerate(((wg_hbm, wg), (wu_hbm, wu), (wd_hbm, wd)))
    ]
    for load in loads:
        load.start()

    barrier = pltpu.get_barrier_semaphore()

    def greet(e, _):
        @pl.when(e != me)
        def _():
            pl.semaphore_signal(barrier, inc=1, device_id=(e, y), device_id_type=MESH)

        return 0

    lax.fori_loop(0, experts, greet, 0)
    for other in (right, left, far):
        pl.semaphore_signal(barrier, inc=1, device_id=(me, other), device_id_type=MESH)

    distances = sum((d % nz) << (4 * k) for k, d in enumerate(DISTANCE[:groups]))

    def step_of(g):
        if isinstance(g, int):
            return DISTANCE[g] % nz
        return lax.rem(lax.shift_right_logical(jnp.int32(distances), 4 * g), 16)

    def other_j(o):
        return lax.rem(x + o // CORES, nx) * CORES + lax.rem(core + o % CORES, CORES)

    def tile(e):
        return pl.ds(pl.multiple_of(e * MAIN, MAIN), MAIN)

    rank[...] = ranks(routes[...], experts)
    expert = iota((experts, count), 0)
    weight_of = jnp.zeros((experts, count), F32)
    for k in range(routes.shape[0]):
        weight_of = weight_of + jnp.where(routes[k : k + 1, :] == expert, weights[k : k + 1, :], 0.0)
    weight[...] = weight_of
    loads[0].wait()
    loads[1].wait()

    row = iota((main, count), 0)
    quarter = lax.div(lax.rem(iota((main, piece), 0), MAIN), REST)
    own_columns = pl.ds(pl.multiple_of(y * width, width), width)

    def pickers(g):
        zd = lax.rem(z + step_of(g), nz)
        at = pl.ds(pl.multiple_of(zd * nj, nj), nj)
        rk = jnp.broadcast_to(rank[at, :][:, None, :], (nj, MAIN, count)).reshape(main, count)
        wt = jnp.broadcast_to(weight[at, :][:, None, :], (nj, MAIN, count)).reshape(main, count)
        out = []
        for slot in (lax.rem(row, MAIN) + 1, lax.rem(row, REST) + 1 + MAIN):
            pick = rk == slot.astype(F32)
            hot = jnp.where(pick, 1.0, 0.0).astype(BF16)
            out.append((hot, jnp.sum(jnp.where(pick, wt, 0.0), axis=1, keepdims=True)))
        return out

    def pack(out, values, picks, scaled):
        (hot, scale), (hot_rest, scale_rest) = picks
        body = nn(hot, values)
        tail = nn(hot_rest, values)
        edge = tail[:, 0:piece]
        for q in range(1, REST):
            edge = jnp.where(quarter == q, tail[:, q * piece : (q + 1) * piece], edge)
        if scaled:
            body, edge = body * scale, edge * scale_rest
        out[:, 0:width] = body.astype(BF16)
        out[:, width:packed] = edge.astype(BF16)

    def pack_own(g, _):
        picks = pickers(g)
        pack(s.at[g, 0], x_in[:, own_columns], picks, False)
        pack(s.at[g, 1], dy_in[:, own_columns], picks, True)
        return 0

    def send_own(g):
        zd = lax.rem(z + step_of(g), nz)
        for o in range(nj):
            to = other_j(o)
            dest = zd * nj + to
            if g in NEAR:
                src, dst = s.at[g, 1, tile(to), SPLIT:packed], m.at[g, y, 1, tile(j), SPLIT:packed]
            else:
                src, dst = s.at[g, :, tile(to), :], m.at[g, y, :, tile(j), :]
            remote(src, dst, ep_send, ep_recv.at[g], dest, y).start()

    lax.fori_loop(1, groups, pack_own, 0)
    pl.semaphore_wait(barrier, experts - 1 + 3)
    for g in (6, 7, 1, 2):
        send_own(g)

    picks = pickers(0)
    for slab in range(ny):
        pack(s_here.at[slab, 0], x_in[:, slab * width : (slab + 1) * width], picks, False)
        pack(s_here.at[slab, 1], dy_in[:, slab * width : (slab + 1) * width], picks, True)
    for o in range(1, nj):
        to = other_j(o)
        remote(
            s_here.at[:, :, tile(to), :], m.at[0, :, :, tile(j), :], ep_send, ep_recv.at[0], z * nj + to, y
        ).start()
    for slab in range(ny):
        for k in range(2):
            m[0, slab, k, tile(j), :] = s_here[slab, k, tile(j), :]
    for g in (3, 4, 5):
        send_own(g)
    for n, g in enumerate(NEAR):
        picks = pickers(g)
        for slab in range(ny):
            c0 = slab * width
            pack(s_near.at[n, slab], x_in[:, c0 : c0 + width], picks, False)
            hot, scale = picks[0]
            s_edge[n, slab] = (nn(hot, dy_in[:, c0 : c0 + SPLIT]) * scale).astype(BF16)
        zd = lax.rem(z + step_of(g), nz)
        for o in range(nj):
            to = other_j(o)
            dest = zd * nj + to
            src, dst = s_near.at[n, :, tile(to), :], m.at[g, :, 0, tile(j), :]
            remote(src, dst, near_send, near_recv.at[0, n], dest, y).start()
            src, dst = s_edge.at[n, :, tile(to), :], m.at[g, :, 1, tile(j), 0:SPLIT]
            remote(src, dst, near_send, near_recv.at[1, n], dest, y).start()

    a, b = iota((main, main), 0), iota((main, main), 1)
    q_of, src_of, j_of = lax.div(a, rest), lax.div(lax.rem(a, rest), REST), lax.rem(a, REST)
    apart = jnp.where(b == src_of * MAIN + q_of * REST + j_of, 1.0, 0.0).astype(BF16)
    q_in, src_in, j_in = lax.div(b, rest), lax.div(lax.rem(b, rest), REST), lax.rem(b, REST)
    together = jnp.where(a == src_in * MAIN + q_in * REST + j_in, 1.0, 0.0).astype(BF16)
    r, lane = iota((rows, 128), 0), iota((rows, 128), 1)
    slot_of = jnp.where(r < main, lax.rem(r, MAIN), MAIN + lax.rem(r, REST))
    at_slot = lane == slot_of
    rr = iota((nj, rows), 1)
    from_src = jnp.where(rr < main, lax.div(rr, MAIN), lax.div(rr - main, REST)) == iota((nj, rows), 0)
    from_src = jnp.where(from_src, 1.0, 0.0)

    def part(g, slab):
        return m.at[g, slab, 1, :, SPLIT:packed] if g in NEAR else m.at[g, slab]

    def halves(g, slab):
        if g in NEAR:
            return [m.at[g, slab, 1, pl.ds(h * half_main, half_main), SPLIT:packed] for h in range(2)]
        return [m.at[g, slab, :, pl.ds(h * half_main, half_main), :] for h in range(2)]

    def arrive(g):
        await_bytes(part(g, y), ep_recv.at[g])
        remote(part(g, y), part(g, y), y_send, y_recv.at[0, g], me, right).start()
        remote(part(g, y), part(g, y), y_send, y_recv.at[1, g], me, left).start()

    def forward(g):
        await_bytes(part(g, left), y_recv.at[0, g])
        low = halves(g, left)[0]
        remote(low, low, f_send, f_recv.at[0, g], me, right).start()
        await_bytes(part(g, right), y_recv.at[1, g])
        high = halves(g, right)[1]
        remote(high, high, f_send, f_recv.at[1, g], me, left).start()

    def gathered(g):
        @pl.when(g == 0)
        def _():
            await_bytes(m.at[0, :, :, pl.ds(0, main - MAIN), :], ep_recv.at[0])
            for load in loads[2:]:
                load.wait()

        for n, near in enumerate(NEAR):

            @pl.when(g == near)
            def _(n=n, near=near):
                await_bytes(m.at[near, :, 0], near_recv.at[0, n])
                await_bytes(m.at[near, :, 1, :, 0:SPLIT], near_recv.at[1, n])
                for h in range(2):
                    await_bytes(halves(near, far)[h], f_recv.at[h, near])

        @pl.when((g != 0) & (g != NEAR[0]) & (g != NEAR[1]))
        def _():
            for h in range(2):
                await_bytes(m.at[g, far, :, pl.ds(h * half_main, half_main), :], f_recv.at[h, g])

    def compute(g):
        gathered(g)
        row0 = pl.multiple_of(g * rows, REST * nj)
        at_main, at_rest, at_all = pl.ds(row0, main), pl.ds(row0 + main, rest), pl.ds(row0, rows)
        for slab in range(ny):
            c0 = slab * width
            for k, out in enumerate((xa, da)):
                out[at_main, c0 : c0 + width] = m[g, slab, k, :, 0:width]
                pieces = nn(apart, m[g, slab, k, :, width:packed]).astype(BF16)
                for q in range(REST):
                    out[at_rest, c0 + q * piece : c0 + (q + 1) * piece] = pieces[q * rest : (q + 1) * rest]
        gate_pre = nn(xa[at_all, :], wg[...])
        up_pre = nn(xa[at_all, :], wu[...])
        hidden_grad = nt(da[at_all, :], wd[...])
        glu = jnp.minimum(gate_pre, LIMIT)
        linear = jnp.clip(up_pre, -LIMIT, LIMIT)
        sigma = jax.nn.sigmoid(SLOPE * glu)
        active = glu * sigma
        hidden = (active * (linear + 1.0)).astype(BF16)
        slope = sigma + SLOPE * active * (1.0 - sigma)
        gpg = jnp.where(gate_pre < LIMIT, hidden_grad * (linear + 1.0) * slope, 0.0).astype(BF16)
        upg = jnp.where(jnp.abs(up_pre) < LIMIT, hidden_grad * active, 0.0).astype(BF16)
        ga[at_all, :] = gpg
        ua[at_all, :] = upg
        ha[at_all, :] = hidden
        for slab in range(ny):
            c0 = slab * width
            term = nt(gpg, wg[c0 : c0 + width, :]) + nt(upg, wu[c0 : c0 + width, :])
            rt[g, slab] = term.astype(BF16)
        low, high = pl.ds(0, half), pl.ds(half, half)
        remote(rt.at[g, far, low], ra.at[g, 0], ra_send, ra_recv.at[0, g], me, right).start()
        remote(rt.at[g, far, high], ra.at[g, 1], ra_send, ra_recv.at[1, g], me, left).start()
        remote(rt.at[g, right, high], rb.at[g, 0, high], rb_send, rb_recv.at[0, g], me, right).start()
        remote(rt.at[g, left, low], rb.at[g, 1, low], rb_send, rb_recv.at[1, g], me, left).start()
        product = jnp.sum(hidden.astype(F32) * hidden_grad, axis=1, keepdims=True)
        laid = nn(from_src, jnp.where(at_slot, product, 0.0), HIGH)
        for src in range(nj):
            pq[g, src] = laid[src : src + 1, :]
        zs = lax.rem(z - step_of(g) + nz, nz)
        for o in range(nj):
            to = other_j(o)

            def send_products(to=to):
                remote(pq.at[g, to], qin.at[me], q_send, q_recv, zs * nj + to, y).start()

            if o == 0:
                pl.when(g > 0)(send_products)
            else:
                send_products()

    def partly(g):
        low, high = pl.ds(0, half), pl.ds(half, half)
        await_bytes(ra.at[g, 0], ra_recv.at[0, g])
        rc[g, 0] = (ra[g, 0].astype(F32) + rt[g, right, low].astype(F32)).astype(BF16)
        remote(rc.at[g, 0], rb.at[g, 0, low], rb_send, rb_recv.at[0, g], me, right).start()
        await_bytes(ra.at[g, 1], ra_recv.at[1, g])
        rc[g, 1] = (ra[g, 1].astype(F32) + rt[g, left, high].astype(F32)).astype(BF16)
        remote(rc.at[g, 1], rb.at[g, 1, high], rb_send, rb_recv.at[1, g], me, left).start()

    def give_back(g):
        await_bytes(rb.at[g, 0], rb_recv.at[0, g])
        await_bytes(rb.at[g, 1], rb_recv.at[1, g])
        total = rt[g, y].astype(F32) + rb[g, 0].astype(F32) + rb[g, 1].astype(F32)
        done = total.astype(BF16)
        bo[g, :, 0:width] = done[0:main]
        stacked = jnp.concatenate([done[main:rows, q * piece : (q + 1) * piece] for q in range(REST)], axis=0)
        bo[g, :, width:packed] = nn(together, stacked).astype(BF16)
        zs = lax.rem(z - step_of(g) + nz, nz)
        for o in range(nj):
            to = other_j(o)

            def send_rows(to=to):
                remote(bo.at[g, tile(to), :], bk.at[tile(me), :], back_send, back_recv, zs * nj + to, y).start()

            if o == 0:
                pl.when(g > 0)(send_rows)
            else:
                send_rows()

    block = min(256, xa.shape[1])

    def weight_grads(i, _):
        at = pl.ds(pl.multiple_of(i * block, block), block)
        dwg[at, :] = tn(xa[:, at], ga[...])
        dwu[at, :] = tn(xa[:, at], ua[...])
        dwd[:, at] = tn(ha[...], da[:, at])
        pltpu.make_async_copy(dwg.at[at, :], dwg_hbm.at[at, :], dw_sem.at[0]).start()
        pltpu.make_async_copy(dwu.at[at, :], dwu_hbm.at[at, :], dw_sem.at[1]).start()
        pltpu.make_async_copy(dwd.at[:, at], dwd_hbm.at[:, at], dw_sem.at[2]).start()
        return 0

    def step(i, _):
        @pl.when(i == 0)
        def _():
            arrive(6)
            arrive(7)
            forward(6)
            forward(7)
            arrive(1)
            arrive(2)

        @pl.when(i == 1)
        def _():
            forward(1)
            forward(2)
            arrive(3)
            arrive(4)

        pl.when(i == 2)(lambda: forward(3))
        pl.when(i == 3)(lambda: arrive(5))
        pl.when(i == 4)(lambda: forward(5))
        compute(i)
        pl.when(i == 2)(lambda: forward(4))
        pl.when(i >= 1)(lambda: partly(i - 1))
        pl.when(i >= 2)(lambda: give_back(i - 2))
        return 0

    lax.fori_loop(0, groups, step, 0)
    blocks = xa.shape[1] // block
    cuts = (0, blocks * 3 // 8, blocks * 6 // 8, blocks)
    lax.fori_loop(cuts[0], cuts[1], weight_grads, 0)
    partly(groups - 1)
    give_back(groups - 2)
    lax.fori_loop(cuts[1], cuts[2], weight_grads, 0)
    give_back(groups - 1)

    own_copy = pltpu.make_async_copy(bo.at[0, tile(j), :], bk.at[tile(me), :], own_sem)
    own_copy.start()
    qin[me] = pq[0, j]
    await_bytes(qin.at[pl.ds(0, experts - 1)], q_recv)
    remote(qin, qy.at[0], qy_send.at[0], qy_recv.at[0], me, right).start()
    remote(qin, qy.at[1], qy_send.at[1], qy_recv.at[1], me, left).start()
    remote(qin, qy.at[2], qy_send.at[2], qy_recv.at[2], me, far).start()

    lax.fori_loop(cuts[2], cuts[3], weight_grads, 0)

    for k in range(3):
        await_bytes(qy.at[k], qy_recv.at[k])
        await_bytes(qin, qy_send.at[k])
    q_out[...] = qin[...] + qy[0] + qy[1] + qy[2]

    await_bytes(m.at[0:2], ep_send)
    await_bytes(m.at[0, 0, :, 0:half_main, :], ep_send)
    await_bytes(m.at[0, 0:2, 0, :, SPLIT:packed], ep_send)
    await_bytes(m.at[0:2, :, 0], near_send)
    await_bytes(m.at[0:2, :, 1, :, 0:SPLIT], near_send)
    for _ in range(2):
        await_bytes(m.at[0:5, 0], y_send)
        await_bytes(m.at[0:2, 0, 1, :, SPLIT:packed], y_send)
        await_bytes(m.at[0:5, 0, :, 0:half_main, :], f_send)
        await_bytes(m.at[0:2, 0, 1, 0:half_main, SPLIT:packed], f_send)
        await_bytes(ra.at[:, 0], ra_send)
        await_bytes(rb.at[:, 0], rb_send)
    everything = pl.ds(0, (experts - 1) * MAIN)
    await_bytes(bk.at[everything, :], back_send)
    await_bytes(qin.at[pl.ds(0, experts - 1)], q_send)
    own_copy.wait()
    for k, (a, b) in enumerate(((dwg, dwg_hbm), (dwu, dwu_hbm), (dwd, dwd_hbm))):
        pltpu.make_async_copy(a, b, dw_sem.at[k]).wait()
    await_bytes(bk.at[everything, :], back_recv)


def finish_kernel(
    experts, routes_ref, weights_ref, bk_in, q_in, a_in, b_in, c_in,
    grad_ref, gate_ref, a_out, b_out, c_out,
    bk, q, a, b, c, first_sem, in_sem, out_sem,
):
    parts = in_sem.shape[1]
    load_bk = pltpu.make_async_copy(bk_in, bk, first_sem.at[0])
    load_q = pltpu.make_async_copy(q_in, q, first_sem.at[1])
    load_q.start()
    load_bk.start()
    copies = []
    for n, (src, mid, dst) in enumerate(((a_in, a, a_out), (b_in, b, b_out), (c_in, c, c_out))):
        size = src.shape[0] // parts
        for k in range(parts):
            at = pl.ds(k * size, size)
            first = pltpu.make_async_copy(src.at[at, :], mid.at[at, :], in_sem.at[n, k])
            second = pltpu.make_async_copy(mid.at[at, :], dst.at[at, :], out_sem.at[n, k])
            first.start()
            copies.append((first, second))

    def pass_on(some):
        for first, second in some:
            first.wait()
            second.start()

    routes = routes_ref[...]
    count = routes.shape[1]
    rank = ranks(routes, experts)
    slots = experts * MAIN
    spread = jnp.where(lax.div(iota((experts, slots), 1), MAIN) == iota((experts, slots), 0), 1.0, 0.0).astype(BF16)
    rk = tn(rank.astype(BF16), spread)
    pass_on(copies[:4])
    load_q.wait()
    products = q[...]
    expert = iota((experts, count), 0)
    for k in range(routes.shape[0]):
        mine = routes[k : k + 1, :] == expert
        slot = jnp.sum(jnp.where(mine, rank, 0.0), axis=0, keepdims=True)
        found = tn(products, jnp.where(mine, 1.0, 0.0), HIGH)
        chosen = jnp.where(iota(found.shape, 0).astype(F32) + 1.0 == slot, found, 0.0)
        gate_ref[k : k + 1, :] = jnp.sum(chosen, axis=0, keepdims=True) / weights_ref[k : k + 1, :]
    pass_on(copies[4:12])
    lane = lax.rem(iota((count, slots), 1), MAIN)
    width = bk.shape[1] * REST // (REST + 1)
    piece = width // REST
    hot = jnp.where(rk == lane.astype(F32) + 1.0, 1.0, 0.0).astype(BF16)
    load_bk.wait()
    total = nn(hot, bk[:, 0:width])
    pass_on(copies[12:18])
    late = rk == lax.rem(lane, REST).astype(F32) + (1.0 + MAIN)
    for n in range(REST):
        hot = jnp.where(late & (lax.div(lane, REST) == n), 1.0, 0.0).astype(BF16)
        at = slice(n * piece, (n + 1) * piece)
        grad_ref[:, at] = (total[:, at] + nn(hot, bk[:, width : width + piece])).astype(BF16)
    pass_on(copies[18:])
    for _, second in copies:
        second.wait()


def local(nz, nj, ny, tokens, routes, gate_weights, out_grad, w_gate, w_up, w_down):
    count, model = tokens.shape
    units = w_gate.shape[2]
    top = routes.shape[1]
    experts = nz * nj
    width = model // ny
    packed = width * (REST + 1) // REST
    vmem = pl.BlockSpec(memory_space=pltpu.VMEM)
    hbm = pl.BlockSpec(memory_space=pltpu.HBM)
    routes_t, weights_t = routes.T, gate_weights.T

    groups, main, rows = nz, nj * MAIN, nj * (MAIN + REST)
    all_rows = groups * rows
    dma = pltpu.SemaphoreType.DMA
    weight_shapes = (
        jax.ShapeDtypeStruct((model, units), F32),
        jax.ShapeDtypeStruct((model, units), F32),
        jax.ShapeDtypeStruct((units, model), F32),
    )
    back, products, dwg, dwu, dwd = pl.pallas_call(
        functools.partial(exchange_kernel, nz, nj, ny),
        out_shape=(
            jax.ShapeDtypeStruct((experts * MAIN, packed), BF16),
            jax.ShapeDtypeStruct((experts, 1, 128), F32),
            *weight_shapes,
        ),
        in_specs=[vmem, vmem] + [hbm] * 5,
        out_specs=(hbm, vmem, hbm, hbm, hbm),
        scratch_shapes=[
            pltpu.VMEM((count, model), BF16),
            pltpu.VMEM((count, model), BF16),
            pltpu.VMEM((model, units), BF16),
            pltpu.VMEM((model, units), BF16),
            pltpu.VMEM((units, model), BF16),
            pltpu.VMEM((experts, count), F32),
            pltpu.VMEM((experts, count), F32),
            pltpu.VMEM((groups, 2, main, packed), BF16),
            pltpu.VMEM((len(NEAR), ny, main, packed), BF16),
            pltpu.VMEM((len(NEAR), ny, main, SPLIT), BF16),
            pltpu.VMEM((ny, 2, main, packed), BF16),
            pltpu.VMEM((groups, ny, 2, main, packed), BF16),
            pltpu.VMEM((all_rows, model), BF16),
            pltpu.VMEM((all_rows, model), BF16),
            pltpu.VMEM((all_rows, units), BF16),
            pltpu.VMEM((all_rows, units), BF16),
            pltpu.VMEM((all_rows, units), BF16),
            pltpu.VMEM((groups, ny, rows, width), BF16),
            pltpu.VMEM((groups, 2, rows // 2, width), BF16),
            pltpu.VMEM((groups, 2, rows, width), BF16),
            pltpu.VMEM((groups, 2, rows // 2, width), BF16),
            pltpu.VMEM((groups, main, packed), BF16),
            pltpu.VMEM((groups, nj, 1, 128), F32),
            pltpu.VMEM((experts, 1, 128), F32),
            pltpu.VMEM((3, experts, 1, 128), F32),
            *(pltpu.VMEM(w.shape, F32) for w in weight_shapes),
            dma((2,)), dma((3,)), dma, dma((3,)),
            dma, dma((groups,)),
            dma, dma((2, len(NEAR))),
            dma, dma((2, groups)),
            dma, dma((2, groups)),
            dma, dma((2, groups)),
            dma, dma((2, groups)),
            dma, dma,
            dma, dma,
            dma((3,)), dma((3,)),
        ],
        compiler_params=pltpu.CompilerParams(
            collective_id=0, has_side_effects=True, vmem_limit_bytes=67_043_328
        ),
        name="exchange",
    )(routes_t, weights_t, tokens, out_grad, w_gate[0], w_up[0], w_down[0])

    token_grad, gate_grad, dwg, dwu, dwd = pl.pallas_call(
        functools.partial(finish_kernel, experts),
        out_shape=(
            jax.ShapeDtypeStruct((count, width), BF16),
            jax.ShapeDtypeStruct((top, count), F32),
            *weight_shapes,
        ),
        in_specs=[vmem] * 2 + [hbm] * 5,
        out_specs=(vmem, vmem, hbm, hbm, hbm),
        scratch_shapes=[
            pltpu.VMEM((experts * MAIN, packed), BF16),
            pltpu.VMEM((experts, 128), F32),
            *(pltpu.VMEM(w.shape, F32) for w in weight_shapes),
            dma((2,)), dma((3, 8)), dma((3, 8)),
        ],
        compiler_params=pltpu.CompilerParams(vmem_limit_bytes=67_043_328),
        name="finish",
    )(routes_t, weights_t, back, products.reshape(experts, 128), dwg, dwu, dwd)
    return token_grad, gate_grad.T, dwg[None], dwu[None], dwd[None]


def solution(mesh):
    nj = CHIPS_X * CORES
    nz, ny = mesh.shape["ep"] // nj, mesh.shape["tp"]
    in_specs = (
        P("ep", None),
        P("ep", None),
        P("ep", None),
        P("ep", None),
        P("ep", None, "tp"),
        P("ep", None, "tp"),
        P("ep", "tp", None),
    )
    out_specs = (P("ep", "tp"), P("ep", None), P("ep", None, "tp"), P("ep", None, "tp"), P("ep", "tp", None))
    return jax.shard_map(
        functools.partial(local, nz, nj, ny), mesh=mesh, in_specs=in_specs, out_specs=out_specs, check_vma=False
    )
```
